1024 devices in a mesh: ep: 32 (over z, core), tp: 32 (over y, x).
Axes of the slice: x: 4, y: 8, z: 16, core: 2. Of those that a mesh axis runs over, the one named last changes fastest.
Arguments:
- resid: bfloat16 [1024, 2048], P('ep', 'tp'), may hold values from -6 to 6
- cache_key: bfloat16 [1024, 8, 224, 256], P(('ep', 'tp')), may hold values from -360 to 360
- cache_value: bfloat16 [1024, 8, 224, 256], P(('ep', 'tp')), may hold values from -6 to 6
- lengths: int32 [1024], P(('ep', 'tp')), may hold values from 28 to 224
- lambdas: float32 [8], replicated, may hold values from 0.3 to 0.8
- mix_gain: float32 [2048], replicated, may hold values from 0.1 to 1.9
- query_gain: float32 [128], replicated, may hold values from 0.1 to 1.9
- key_gain: float32 [128], replicated, may hold values from 0.1 to 1.9
- sub_gain: float32 [256], replicated, may hold values from 0.1 to 1.9
- ffn_gain: float32 [2048], replicated, may hold values from 0.1 to 1.9
- w_query: bfloat16 [2048, 2048], P(None, 'tp'), may hold values from -0.125 to 0.125
- w_key: bfloat16 [2048, 2048], P(None, 'tp'), may hold values from -0.125 to 0.125
- w_value: bfloat16 [2048, 2048], P(None, 'tp'), may hold values from -0.125 to 0.125
- w_out: bfloat16 [2048, 2048], P(None, 'tp'), may hold values from -0.125 to 0.125
- routes: int32 [1024, 2], P('ep'), may hold values from 0 to 31, all different within a row; in each aligned block of 32 rows (0 to 31, 32 to 63, ...) at most 4 rows name the same one
- route_weights: float32 [1024, 2], P('ep'), may hold values from 0.2 to 0.8
- w_gate: bfloat16 [32, 2048, 4096], P('ep', None, 'tp'), may hold values from -0.125 to 0.125
- w_up: bfloat16 [32, 2048, 4096], P('ep', None, 'tp'), may hold values from -0.125 to 0.125
- w_down: bfloat16 [32, 4096, 2048], P('ep', 'tp'), may hold values from -0.09375 to 0.09375
Outputs:
- result: bfloat16 [1024, 2048], P('ep', 'tp')
- new_key: bfloat16 [1024, 8, 256], P(('ep', 'tp'))
- new_value: bfloat16 [1024, 8, 256], P(('ep', 'tp'))
The draws below stay inside these ranges and needn't reach their ends.
Inputs may be any that keep to these rules, and one draw needn't show every extreme that they name: `routes`: within the 32 rows of one index of ep no expert is named more than 4 times, and in some of them one expert is named exactly 4 times; the two experts of a row differ. `lengths`: every sequence has at least two live positions.
All inputs are finite; a program needn't handle non-finite values.
Results may differ from the reference program's by a relative error of at most 0.0099.
Values may be sent and summed in bfloat16 or wider, within the bound.
No kernel may reach another device: no remote copies, remote signals or barrier semaphores. Data moves between devices by JAX's collectives and lax.ppermute only.
A program may use at most 32 MiB of HBM per device.

```python
import functools
import math
import jax
import jax.numpy as jnp
import numpy as np
from jax import lax

D = 2048
HEADS = 8
KVH = 8
DH = 128
VD = 256
QW = 2048
KW = 2048
VW = 2048
OW = 2048
FFE = 4096
CAP = 4
LEN = 224
GROUP = 32
SEQS = 1024
EXPERTS = 32
N_EP = 32


def draw_cache_key(key, part):
    drawn = jnp.clip(1.75 * jax.random.normal(key, (SEQS, KVH, LEN, 2 * DH), jnp.float32), -12.0, 12.0)
    return drawn.astype(jnp.bfloat16)


def set_ends(drawn, key, low, top_value):
    shape = drawn.shape
    index_at = [jax.random.randint(jax.random.fold_in(key, axis), (), 0, shape[axis]) for axis in range(len(shape))]
    drawn = drawn.at[tuple(index_at)].set(low)
    longest = shape.index(max(shape))
    index_at[longest] = (index_at[longest] + 1) % shape[longest]
    return drawn.at[tuple(index_at)].set(top_value)


def levels(key, dims, cuts, least, largest):
    factor_of, own = 1.0, jax.random.fold_in(key, 6)
    for axis_at, blocks in cuts:
        steps = jnp.exp(jax.random.uniform(jax.random.fold_in(own, axis_at), (blocks,), jnp.float32, least / len(cuts), largest / len(cuts)))
        factor_of = factor_of * jnp.repeat(steps, dims[axis_at] // blocks).reshape([-1 if axis == axis_at else 1 for axis in range(len(dims))])
    return factor_of


def shared_out(own_key, own, number, rows, amount, top, bound, skew):
    ranking = jax.random.permutation(own_key, amount)
    heavy_load, common = portions_of(amount, rows * top, bound, skew, True), portions_of(amount, rows * top, bound, skew, False)
    places = jnp.arange(amount)

    def named(sizes, rotation):
        used = int((sizes > 0).sum())
        fixed = max(1, used // 4)
        shifted = fixed + (places - fixed + rotation * (used - fixed)) % max(1, amount - fixed)
        return jnp.zeros((amount,), jnp.int32).at[ranking[jnp.where(places < fixed, places, shifted)]].set(jnp.asarray(sizes, jnp.int32))

    sizes = jnp.where(number % 4 == 0, named(heavy_load, number // 4), named(common, number - number // 4 - 1))
    mixed = jax.random.permutation(jax.random.fold_in(own, 3), amount)
    giver, sink = mixed[0:amount // 2 * 2:2], mixed[1:amount // 2 * 2:2]
    slack = jnp.minimum(sizes[giver] - 1, bound - sizes[sink]) // 2
    slack = jnp.where((giver == ranking[0]) | (sink == ranking[0]) | (sizes[sink] == 0), 0, jnp.maximum(slack, 0))
    shifted = jax.random.randint(jax.random.fold_in(own, 4), (amount // 2,), 0, 1 << 20) % (slack + 1)
    sizes = sizes.at[giver].add(-shifted).at[sink].add(shifted)
    members = jnp.searchsorted(jnp.cumsum(sizes), jnp.arange(rows * top), side="right").astype(jnp.int32)
    listing = members.reshape(top, rows).T
    listing = listing[jax.random.permutation(jax.random.fold_in(own, 1), rows)]
    rotation = jax.random.randint(jax.random.fold_in(own, 2), (rows, 1), 0, top)
    return jnp.take_along_axis(listing, (jnp.arange(top)[None, :] + rotation) % top, axis=1)


def portions_of(amount, total, bound, slope, full):
    weights = [(1 << 20) // math.isqrt(grade ** slope) + 1 for grade in range(1, amount + 1)]
    largest = bound if full else min(bound, max(-(-total // amount), total * weights[0] // sum(weights)))
    least = 1 if total - largest >= amount - 1 else 0
    counts, rest = [largest] + [least] * (amount - 1), total - largest - least * (amount - 1)
    while rest > 0:
        candidates = [i for i in range(1, amount) if counts[i] < largest] or [i for i in range(1, amount) if counts[i] < bound]
        pool, remaining = sum([weights[i] for i in candidates]), rest
        for i in candidates:
            addition = min(bound - counts[i], max(1, remaining * weights[i] // pool), rest)
            counts[i] = counts[i] + addition
            rest = rest - addition
    return np.array(counts)


def gaussian(key, extent, deviation, reach, shards=(), held_as=jnp.bfloat16):
    values = deviation * jax.random.normal(key, extent, jnp.float32)
    if shards:
        values = values * levels(key, extent, shards, -0.22, 0.18)
    return jnp.clip(values, -reach, reach).astype(held_as)


def setup_inputs(seed: int = 0) -> dict:
    splits = jax.random.split(jax.random.key(seed), 20)
    resid = gaussian(splits[0], (SEQS, D), 1.0, 6.0, ((0, 32), (1, 32)))
    cache_key = draw_cache_key(jax.random.fold_in(splits[19], 71), 0)
    cache_value = gaussian(splits[2], (SEQS, KVH, LEN, VD), 1.0, 6.0, ((0, 1024),))
    lengths = set_ends(jax.random.randint(splits[3], (SEQS,), LEN // 8, LEN + 1), jax.random.fold_in(splits[3], 1), LEN // 8, LEN).astype(jnp.int32)
    lambdas = jnp.clip(jax.random.uniform(splits[4], (HEADS,), jnp.float32, 0.3, 0.8), 0.3, 0.8)
    mix_gain = jnp.clip(1.0 + 0.18 * jax.random.normal(splits[5], (D,), jnp.float32), 0.1, 1.9)
    query_gain = jnp.clip(1.0 + 0.18 * jax.random.normal(splits[6], (DH,), jnp.float32), 0.1, 1.9)
    key_gain = jnp.clip(1.0 + 0.18 * jax.random.normal(splits[7], (DH,), jnp.float32), 0.1, 1.9)
    sub_gain = jnp.clip(1.0 + 0.18 * jax.random.normal(splits[8], (VD,), jnp.float32), 0.1, 1.9)
    ffn_gain = jnp.clip(1.0 + 0.18 * jax.random.normal(splits[9], (D,), jnp.float32), 0.1, 1.9)
    w_query = gaussian(splits[10], (D, QW), D ** -0.5, 0.125, ((1, 32),))
    w_key = gaussian(splits[11], (D, KW), D ** -0.5, 0.125, ((1, 32),))
    w_value = gaussian(splits[12], (D, VW), D ** -0.5, 0.125, ((1, 32),))
    w_out = gaussian(splits[13], (OW, D), OW ** -0.5, 0.125, ((1, 32),))
    routes_keys = jax.random.split(jax.random.fold_in(splits[14], 1), SEQS // GROUP)
    routes_turns = jax.random.permutation(jax.random.fold_in(splits[14], 3), SEQS // GROUP)
    routes = jax.vmap(lambda own, number: shared_out(jax.random.fold_in(splits[14], 2), own, number, GROUP, EXPERTS, 2, CAP, 2))(routes_keys, routes_turns).reshape((SEQS, 2))
    route_weights = jnp.clip(0.2 + 0.6 * jax.random.uniform(splits[15], (SEQS, 2), jnp.float32) ** levels(splits[15], (SEQS, 2), ((0, 32),), -0.2, 0.2), 0.2, 0.8)
    w_gate = gaussian(splits[16], (EXPERTS, D, FFE), D ** -0.5, 0.125, ((0, 32), (2, 32)))
    w_up = gaussian(splits[17], (EXPERTS, D, FFE), D ** -0.5, 0.125, ((0, 32), (2, 32)))
    w_down = gaussian(splits[18], (EXPERTS, FFE, D), FFE ** -0.5, 0.09375, ((0, 32), (1, 32)))
    return {"resid": resid, "cache_key": cache_key, "cache_value": cache_value, "lengths": lengths, "lambdas": lambdas, "mix_gain": mix_gain, "query_gain": query_gain, "key_gain": key_gain, "sub_gain": sub_gain, "ffn_gain": ffn_gain, "w_query": w_query, "w_key": w_key, "w_value": w_value, "w_out": w_out, "routes": routes, "route_weights": route_weights, "w_gate": w_gate, "w_up": w_up, "w_down": w_down}


epsilon = 1e-06
out_factor = 0.2 + 0.6 * math.exp(-0.3)
masked_score = -1e+30

def scaled_rows(values, gain):
    wide = values.astype(jnp.float32)
    return wide * lax.rsqrt(lax.optimization_barrier(jnp.mean(wide * wide, axis=-1, keepdims=True)) + epsilon) * gain

def route_tables(routes, route_weights, experts, capacity):
    flat_routes = routes.reshape(-1)
    expert_hit = (flat_routes[:, None] == jnp.arange(experts, dtype=jnp.int32)[None, :]).astype(jnp.int32)
    before = jnp.cumsum(expert_hit, axis=0) - expert_hit
    slot_index = lax.optimization_barrier(jnp.sum(before * expert_hit, axis=1))
    slot_hit = (slot_index[:, None] == jnp.arange(capacity, dtype=jnp.int32)[None, :]).astype(jnp.float32)
    pair_table = expert_hit.astype(jnp.float32)[:, :, None] * slot_hit[:, None, :]
    pair_table = pair_table.reshape(routes.shape[0], 2, experts, capacity)
    dispatch = lax.optimization_barrier(jnp.sum(pair_table, axis=1))
    combine = lax.optimization_barrier(jnp.sum(pair_table * route_weights[:, :, None, None], axis=1))
    return (dispatch, combine)

def attend(queries, key_rows, value_rows, past_keys, past_values, live_len, lambdas, query_gain, key_gain, sub_gain):
    seq_count, kv_heads, cache_len, key_width = past_keys.shape
    head_dim = key_width // 2
    head_count = lambdas.shape[0]
    group_size = head_count // kv_heads
    value_dim = past_values.shape[-1]
    score_scale = head_dim ** (-0.5)
    highest = lax.Precision.HIGHEST
    q_unit = scaled_rows(queries.reshape(seq_count, kv_heads, group_size, 2, head_dim), query_gain).astype(jnp.bfloat16)
    new_key = scaled_rows(key_rows.reshape(seq_count, kv_heads, 2, head_dim), key_gain).astype(jnp.bfloat16)
    new_value = value_rows.reshape(seq_count, kv_heads, value_dim)
    past_split = past_keys.reshape(seq_count, kv_heads, cache_len, 2, head_dim)
    scores = jnp.einsum('sjgmd,sjlmd->sjgml', q_unit.astype(jnp.float32), past_split.astype(jnp.float32), precision=highest) * score_scale
    own_score = jnp.einsum('sjgmd,sjmd->sjgm', q_unit.astype(jnp.float32), new_key.astype(jnp.float32), precision=highest) * score_scale
    live_mask = jnp.arange(cache_len, dtype=jnp.int32)[None, :] < live_len[:, None]
    scores = jnp.where(live_mask[:, None, None, None, :], scores, masked_score)
    peak = jnp.maximum(lax.optimization_barrier(jnp.max(scores, axis=-1)), own_score)
    past_weight = jnp.exp(scores - peak[..., None])
    own_weight = jnp.exp(own_score - peak)
    totals = lax.optimization_barrier(jnp.sum(past_weight, axis=-1)) + own_weight
    past_prob = past_weight / totals[..., None]
    own_prob = own_weight / totals
    mix_lambda = lambdas.reshape(1, kv_heads, group_size, 1)
    past_mix = (past_prob[..., 0, :] - mix_lambda * past_prob[..., 1, :]).astype(jnp.bfloat16)
    own_mix = (own_prob[..., 0] - mix_lambda[..., 0] * own_prob[..., 1]).astype(jnp.bfloat16)
    head_out = jnp.einsum('sjgl,sjlv->sjgv', past_mix.astype(jnp.float32), past_values.astype(jnp.float32), precision=highest)
    head_out = head_out + own_mix.astype(jnp.float32)[..., None] * new_value.astype(jnp.float32)[:, :, None, :]
    mixed = (scaled_rows(head_out, sub_gain) * out_factor).astype(jnp.bfloat16).reshape(seq_count, head_count * value_dim)
    return (mixed, new_key.reshape(seq_count, kv_heads, key_width), new_value)

def reference(resid, cache_key, cache_value, lengths, lambdas, mix_gain, query_gain, key_gain, sub_gain, ffn_gain, w_query, w_key, w_value, w_out, routes, route_weights, w_gate, w_up, w_down):
    normed = scaled_rows(resid, mix_gain).astype(jnp.bfloat16)
    queries = jnp.dot(normed, w_query, preferred_element_type=jnp.float32).astype(jnp.bfloat16)
    key_rows = jnp.dot(normed, w_key, preferred_element_type=jnp.float32).astype(jnp.bfloat16)
    value_rows = jnp.dot(normed, w_value, preferred_element_type=jnp.float32).astype(jnp.bfloat16)
    block_count = SEQS // GROUP

    def split_blocks(array):
        return array.reshape((block_count, GROUP) + array.shape[1:])

    def one_block(block_args):
        return attend(block_args[0], block_args[1], block_args[2], block_args[3], block_args[4], block_args[5], lambdas, query_gain, key_gain, sub_gain)
    mixed, new_key, new_value = lax.map(one_block, (split_blocks(queries), split_blocks(key_rows), split_blocks(value_rows), split_blocks(cache_key), split_blocks(cache_value), split_blocks(lengths)))
    mixed = mixed.reshape(SEQS, OW)
    updated = (resid.astype(jnp.float32) + jnp.dot(mixed, w_out, preferred_element_type=jnp.float32)).astype(jnp.bfloat16)
    hidden = scaled_rows(updated, ffn_gain).astype(jnp.bfloat16)
    tables = jax.vmap(functools.partial(route_tables, experts=EXPERTS, capacity=CAP))
    dispatch, combine = tables(routes.reshape(N_EP, GROUP, 2), route_weights.reshape(N_EP, GROUP, 2))
    highest = lax.Precision.HIGHEST
    send = jnp.einsum('ngec,ngd->encd', dispatch, hidden.reshape(N_EP, GROUP, D).astype(jnp.float32), precision=highest).astype(jnp.bfloat16)

    def one_expert(expert_args):
        gate_weight, up_weight, down_weight, slots = expert_args
        flat_rows = slots.reshape(N_EP * CAP, D)
        gate_out = jnp.dot(flat_rows, gate_weight, preferred_element_type=jnp.float32)
        up_out = jnp.dot(flat_rows, up_weight, preferred_element_type=jnp.float32)
        act = (jax.nn.silu(gate_out) * up_out).astype(jnp.bfloat16)
        return jnp.dot(act, down_weight, preferred_element_type=jnp.float32).reshape(N_EP, CAP, D)
    outputs = lax.map(one_expert, (w_gate, w_up, w_down, send))
    expert_mix = jnp.einsum('ngec,encd->ngd', combine, outputs, precision=highest).reshape(SEQS, D)
    result = (updated.astype(jnp.float32) + expert_mix).astype(jnp.bfloat16)
    return (result, new_key.reshape(SEQS, KVH, 2 * DH), new_value.reshape(SEQS, KVH, VD))
```

```python
import math

import jax
import jax.numpy as jnp
from jax import lax
from jax.experimental import pallas as pl
from jax.experimental.pallas import tpu as pltpu
from jax.sharding import PartitionSpec as P

CAP = 4
EPS = 1e-06
OUT_FACTOR = 0.2 + 0.6 * math.exp(-0.3)
MASKED = -1e30

f32 = jnp.float32
bf16 = jnp.bfloat16

VMEM = pl.BlockSpec(memory_space=pltpu.VMEM)
SMEM = pl.BlockSpec(memory_space=pltpu.SMEM)


def nt(a, b):
    return lax.dot_general(a, b, (((1,), (1,)), ((), ())), preferred_element_type=f32)


def nn(a, b):
    return lax.dot_general(a, b, (((1,), (0,)), ((), ())), preferred_element_type=f32)


def tn(a, b):
    return lax.dot_general(a, b, (((0,), (0,)), ((), ())), preferred_element_type=f32)


def left_half(shape):
    return lax.broadcasted_iota(jnp.int32, shape, len(shape) - 1) < 64


def swap(x):
    return pltpu.roll(x, 64, 1)


def pack_kernel(x_ref, o_ref):
    x = x_ref[...].astype(f32)
    o_ref[...] = jnp.concatenate([x[:16], x[16:]], axis=1).astype(bf16)


def qkv_kernel(x_ref, gain_ref, wq_ref, wk_ref, wv_ref, o_ref, s_ref):
    tp = x_ref.shape[0] // 16
    left = left_half((16, 128))
    tiles = []
    total = jnp.zeros((32, 128), f32)
    for i in range(tp // 2):
        a = x_ref[32 * i : 32 * i + 16, :].astype(f32)
        b = x_ref[32 * i + 16 : 32 * i + 32, :].astype(f32)
        tile = jnp.concatenate(
            [jnp.where(left, a, swap(b)), jnp.where(left, swap(a), b)], axis=0
        )
        total = total + tile * tile
        tiles.append(tile)
    width = 64.0 * tp
    scale = lax.rsqrt(jnp.sum(total, axis=1, keepdims=True) / width + EPS)
    normed = jnp.concatenate(
        [(tile * scale * gain_ref[i : i + 1, :]).astype(bf16) for i, tile in enumerate(tiles)],
        axis=1,
    )
    q = nt(normed, wq_ref[...])
    k = nt(normed, wk_ref[...])
    v = nt(normed, wv_ref[...])
    s_ref[pl.ds(0, 32, stride=2), :] = jnp.concatenate([q, k], axis=1)
    s_ref[pl.ds(1, 32, stride=2), :] = jnp.concatenate([v, jnp.zeros_like(v)], axis=1)
    o_ref[...] = s_ref[...].astype(bf16)


def attend_kernel(
    len_ref, lam_ref, x_ref, ck_ref, cv_ref, qg_ref, kg_ref, sg_ref, o_ref, nk_ref, nv_ref, s_ref, p_ref
):
    heads, length, width = ck_ref.shape
    s_ref[...] = x_ref[...].astype(f32)
    rows = 2 * heads
    qk_even = s_ref[pl.ds(0, rows, stride=4), :]
    v_even = s_ref[pl.ds(1, rows, stride=4), :]
    qk_odd = s_ref[pl.ds(2, rows, stride=4), :]
    v_odd = s_ref[pl.ds(3, rows, stride=4), :]
    left = left_half((rows, 128))
    q = jnp.where(left, qk_even, swap(qk_odd))
    k = jnp.where(left, swap(qk_even), qk_odd)
    v = jnp.where(left, v_even, swap(v_odd))

    def unit(z, gain):
        r = lax.rsqrt(jnp.mean(z * z, axis=1, keepdims=True) + EPS)
        return (z * r * gain).astype(bf16).astype(f32)

    qu = unit(q, qg_ref[...])
    ku = unit(k, kg_ref[...])
    s_ref[0:rows, :] = ku
    s_ref[rows : 2 * rows, :] = v
    new_key = jnp.concatenate(
        [s_ref[pl.ds(0, heads, stride=2), :], s_ref[pl.ds(1, heads, stride=2), :]], axis=1
    )
    new_value = jnp.concatenate(
        [s_ref[pl.ds(rows, heads, stride=2), :], s_ref[pl.ds(rows + 1, heads, stride=2), :]], axis=1
    )
    nk_ref[...] = new_key.astype(bf16)
    nv_ref[...] = new_value.astype(bf16)

    row = lax.broadcasted_iota(jnp.int32, (rows, 1), 0)
    first_map = (row % 2) == 0
    wide = jnp.concatenate(
        [jnp.where(first_map, qu, 0.0), jnp.where(first_map, 0.0, qu)], axis=1
    )
    scores = jnp.zeros((rows, length), f32)
    for h in range(heads):
        lhs = jnp.where(row // 2 == h, wide, 0.0).astype(bf16)
        scores = scores + nt(lhs, ck_ref[h])
    scale = 128.0 ** -0.5
    scores = scores * scale
    own = jnp.sum(qu * ku, axis=1, keepdims=True) * scale
    live = lax.broadcasted_iota(jnp.int32, (rows, length), 1) < len_ref[0]
    scores = jnp.where(live, scores, MASKED)
    peak = jnp.maximum(jnp.max(scores, axis=1, keepdims=True), own)
    weight = jnp.exp(scores - peak)
    own_weight = jnp.exp(own - peak)
    totals = jnp.sum(weight, axis=1, keepdims=True) + own_weight
    prob = weight / totals
    p_ref[0] = prob[:, 0:128]
    p_ref[1] = jnp.concatenate([prob[:, 128:length], jnp.zeros((rows, 256 - length), f32)], axis=1)
    p_ref[2] = jnp.broadcast_to(own_weight / totals, (rows, 128))
    head = lax.broadcasted_iota(jnp.int32, (heads, 1), 0)
    lam = jnp.zeros((heads, 1), f32)
    for h in range(heads):
        lam = jnp.where(head == h, lam_ref[h], lam)
    mixes = [
        p_ref[pl.ds(j, 1), pl.ds(0, heads, stride=2), :][0] - lam * p_ref[pl.ds(j, 1), pl.ds(1, heads, stride=2), :][0]
        for j in range(3)
    ]
    past_mix = jnp.concatenate(mixes[:2], axis=1)[:, 0:length]
    own_mix = mixes[2][:, 0:1].astype(bf16).astype(f32)
    out = own_mix * new_value.astype(bf16).astype(f32)
    for h in range(heads):
        lhs = jnp.where(head == h, past_mix, 0.0).astype(bf16)
        out = out + nn(lhs, cv_ref[h])
    r = lax.rsqrt(jnp.mean(out * out, axis=1, keepdims=True) + EPS)
    o_ref[...] = (out * r * sg_ref[...] * OUT_FACTOR).astype(bf16)


def slot_table(routes_ref, experts, rows):
    hit_row = jnp.concatenate([routes_ref[0:1, :], routes_ref[1:2, :]], axis=1)
    pairs = hit_row.shape[1]
    hit = (lax.broadcasted_iota(jnp.int32, (experts, pairs), 0) == hit_row).astype(f32)
    upper = (
        lax.broadcasted_iota(jnp.int32, (pairs, pairs), 0)
        < lax.broadcasted_iota(jnp.int32, (pairs, pairs), 1)
    ).astype(bf16)
    before = nn(hit.astype(bf16), upper)
    slot = jnp.sum(before * hit, axis=0, keepdims=True).astype(jnp.int32)
    place = hit_row * 2 + slot // 2
    at = lax.broadcasted_iota(jnp.int32, (rows, pairs), 0) == place
    return [(at & (slot % 2 == half)).astype(f32) for half in (0, 1)]


def project_kernel(x_ref, w_ref, r_ref, routes_ref, u_ref, o_ref, s_ref):
    seqs = r_ref.shape[0]
    heads = x_ref.shape[0] // seqs
    width = x_ref.shape[1]
    for j in range(2):
        s_ref[j] = x_ref[:, 128 * j : 128 * (j + 1)].astype(f32)
    acc = r_ref[...].astype(f32)
    mixed = jnp.concatenate(
        [
            s_ref[pl.ds(j, 1), pl.ds(h, seqs, stride=heads), :][0].astype(bf16)
            for h in range(heads)
            for j in range(2)
        ],
        axis=1,
    )
    acc = acc + nt(mixed, w_ref[...])
    updated = acc.astype(bf16)
    u_ref[...] = updated
    rows = o_ref.shape[0]
    tables = slot_table(routes_ref, rows // 2, rows)
    halves = [nn((t[:, :seqs] + t[:, seqs:]).astype(bf16), updated) for t in tables]
    o_ref[...] = jnp.concatenate(halves, axis=1).astype(bf16)


def expert_kernel(x_ref, gain_ref, wg_ref, wu_ref, wd_ref, o_ref):
    rows = 64
    tp = x_ref.shape[0] // rows
    left = left_half((rows, 128))
    tiles = []
    total = jnp.zeros((2 * rows, 128), f32)
    for i in range(tp // 2):
        a = x_ref[2 * rows * i : 2 * rows * i + rows, :].astype(f32)
        b = x_ref[2 * rows * i + rows : 2 * rows * (i + 1), :].astype(f32)
        tile = jnp.concatenate(
            [jnp.where(left, a, swap(b)), jnp.where(left, swap(a), b)], axis=0
        )
        total = total + tile * tile
        tiles.append(tile)
    scale = lax.rsqrt(jnp.sum(total, axis=1, keepdims=True) / (64.0 * tp) + EPS)
    hidden = jnp.concatenate(
        [(tile * scale * gain_ref[i : i + 1, :]).astype(bf16) for i, tile in enumerate(tiles)],
        axis=1,
    )
    gate = nn(hidden, wg_ref[...])
    up = nn(hidden, wu_ref[...])
    act = (gate / (1.0 + jnp.exp(-gate)) * up).astype(bf16)
    for i in range(tp // 2):
        out = nn(act, wd_ref[:, 128 * i : 128 * (i + 1)])
        a = out[:rows]
        b = out[rows:]
        o_ref[2 * rows * i : 2 * rows * i + rows, :] = jnp.where(left, a, swap(b)).astype(bf16)
        o_ref[2 * rows * i + rows : 2 * rows * (i + 1), :] = jnp.where(left, swap(a), b).astype(bf16)


def sum_kernel(x_ref, o_ref):
    total = jnp.zeros(o_ref.shape, f32)
    rows = o_ref.shape[0]
    for i in range(x_ref.shape[0] // rows):
        total = total + x_ref[rows * i : rows * (i + 1), :].astype(f32)
    o_ref[...] = total.astype(bf16)


def combine_kernel(x_ref, u_ref, routes_ref, rw_ref, o_ref):
    rows = x_ref.shape[0]
    seqs = u_ref.shape[0]
    tables = slot_table(routes_ref, rows // 2, rows)
    x = x_ref[...]
    picked = tn(tables[0].astype(bf16), x[:, :64]) + tn(tables[1].astype(bf16), x[:, 64:])
    out = u_ref[...].astype(f32) + (
        rw_ref[:, 0:1] * picked[:seqs] + rw_ref[:, 1:2] * picked[seqs:]
    )
    o_ref[...] = out.astype(bf16)


def call(body, out, specs, scratch=(), name=None):
    return pl.pallas_call(
        body,
        out_shape=out,
        in_specs=specs,
        out_specs=jax.tree.map(lambda _: VMEM, out),
        scratch_shapes=scratch,
        compiler_params=pltpu.CompilerParams(vmem_limit_bytes=16 * 1024 * 1024),
        name=name,
    )


def sds(shape, dtype=bf16):
    return jax.ShapeDtypeStruct(shape, dtype)


def gather(x, axis):
    n = lax.axis_size(axis)
    copies = jnp.broadcast_to(x, (n, *x.shape))
    out = lax.all_to_all(copies, axis, split_axis=0, concat_axis=0, tiled=True)
    return out.reshape(n * x.shape[0], x.shape[1])


def exchange(x, axis):
    n = lax.axis_size(axis)
    rows, lanes = x.shape
    out = lax.all_to_all(
        x.reshape(n, rows // n, lanes), axis, split_axis=0, concat_axis=0, tiled=True
    )
    return out.reshape(rows, lanes)


def local(
    resid, cache_key, cache_value, lengths, lambdas, mix_gain, query_gain, key_gain, sub_gain,
    ffn_gain, w_query, w_key, w_value, w_out, routes, route_weights, w_gate, w_up, w_down,
):
    routes_t = routes.T
    packed = call(pack_kernel, sds((16, 128)), [VMEM], name="pack")(resid)
    everyone = gather(packed, "tp")
    qkv = call(
        qkv_kernel, sds((64, 128)), [VMEM] * 5, [pltpu.VMEM((64, 128), f32)], name="qkv"
    )(everyone, mix_gain.reshape(16, 128), w_query.T, w_key.T, w_value.T)
    mine = exchange(qkv, "tp")
    mixed, new_key, new_value = call(
        attend_kernel,
        (sds((8, 256)), sds((8, 256)), sds((8, 256))),
        [SMEM, SMEM] + [VMEM] * 6,
        [pltpu.VMEM((64, 128), f32), pltpu.VMEM((3, 16, 128), f32)],
        name="attend",
    )(
        lengths, lambdas, mine, cache_key[0], cache_value[0],
        query_gain.reshape(1, 128), key_gain.reshape(1, 128), sub_gain.reshape(1, 256),
    )
    heads = gather(mixed, "tp")
    updated, send = call(
        project_kernel,
        (sds((32, 64)), sds((64, 128))),
        [VMEM] * 4,
        [pltpu.VMEM((2, 256, 128), f32)],
        name="project",
    )(heads, w_out.T, resid, routes_t)
    slots = exchange(send, "ep")
    slot_rows = gather(slots, "tp")
    partial = call(expert_kernel, sds((2048, 128)), [VMEM] * 5, name="expert")(
        slot_rows, ffn_gain.reshape(16, 128), w_gate[0], w_up[0], w_down[0]
    )
    arrived = exchange(partial, "tp")
    summed = call(sum_kernel, sds((64, 128)), [VMEM], name="sum")(arrived)
    returned = exchange(summed, "ep")
    result = call(combine_kernel, sds((32, 64)), [VMEM] * 4, name="combine")(
        returned, updated, routes_t, route_weights
    )
    return (result, new_key[None], new_value[None])


def solution(mesh):
    in_specs = (
        P("ep", "tp"),
        P(("ep", "tp"), None, None, None),
        P(("ep", "tp"), None, None, None),
        P(("ep", "tp")),
        P(), P(), P(), P(), P(), P(),
        P(None, "tp"),
        P(None, "tp"),
        P(None, "tp"),
        P(None, "tp"),
        P("ep", None),
        P("ep", None),
        P("ep", None, "tp"),
        P("ep", None, "tp"),
        P("ep", "tp", None),
    )
    out_specs = (P("ep", "tp"), P(("ep", "tp"), None, None), P(("ep", "tp"), None, None))
    return jax.shard_map(local, mesh=mesh, in_specs=in_specs, out_specs=out_specs, check_vma=False)
```

```python
import math

import jax
import jax.numpy as jnp
from jax import lax
from jax.experimental import pallas as pl
from jax.experimental.pallas import tpu as pltpu
from jax.sharding import PartitionSpec as P

CAP = 4
EPS = 1e-06
OUT_FACTOR = 0.2 + 0.6 * math.exp(-0.3)
MASKED = -1e30

f32 = jnp.float32
bf16 = jnp.bfloat16

VMEM = pl.BlockSpec(memory_space=pltpu.VMEM)
SMEM = pl.BlockSpec(memory_space=pltpu.SMEM)
HBM = pl.BlockSpec(memory_space=pltpu.HBM)


def nt(a, b):
    return lax.dot_general(a, b, (((1,), (1,)), ((), ())), preferred_element_type=f32)


def nn(a, b):
    return lax.dot_general(a, b, (((1,), (0,)), ((), ())), preferred_element_type=f32)


def tn(a, b):
    return lax.dot_general(a, b, (((0,), (0,)), ((), ())), preferred_element_type=f32)


def left_half(shape):
    return lax.broadcasted_iota(jnp.int32, shape, len(shape) - 1) < 64


def swap(x):
    return pltpu.roll(x, 64, 1)


def pack_kernel(x_ref, o_ref):
    x = x_ref[...].astype(f32)
    packed = jnp.concatenate([x[:16], x[16:]], axis=1).astype(bf16)
    for i in range(o_ref.shape[0] // 16):
        o_ref[16 * i : 16 * (i + 1), :] = packed


def as_column(row):
    n = row.shape[1]
    eye = lax.broadcasted_iota(jnp.int32, (n, n), 0) == lax.broadcasted_iota(jnp.int32, (n, n), 1)
    return jnp.sum(jnp.where(eye, row, 0.0), axis=1, keepdims=True)


def stage_kernel(*refs):
    n = (len(refs) - 8) // 2
    len_ref, lam_ref, routes_ref, rw_ref = refs[:4]
    sources, targets = refs[4 : 4 + n], refs[4 + n : 2 + 2 * n]
    disp_ref, comb_ref, w_ref, lamcol_ref, live_ref, sems = refs[2 + 2 * n :]
    width = sources[0].shape[0]
    targets = [targets[0].at[width * i : width * (i + 1), :] for i in range(3)] + list(targets[1:])
    copies = [
        pltpu.make_async_copy(src, dst, sems.at[i]) for i, (src, dst) in enumerate(zip(sources, targets))
    ]
    for c in copies:
        c.start()
    experts = disp_ref.shape[1] // 2
    rows = disp_ref.shape[1]
    hit_row = jnp.concatenate([routes_ref[0:1, :], routes_ref[1:2, :]], axis=1)
    pairs = hit_row.shape[1]
    seqs = pairs // 2
    hit = (lax.broadcasted_iota(jnp.int32, (experts, pairs), 0) == hit_row).astype(f32)
    upper = (
        lax.broadcasted_iota(jnp.int32, (pairs, pairs), 0)
        < lax.broadcasted_iota(jnp.int32, (pairs, pairs), 1)
    ).astype(bf16)
    before = nn(hit.astype(bf16), upper)
    slot_row = jnp.sum(before * hit, axis=0, keepdims=True)
    slot = slot_row.astype(jnp.int32)
    place = hit_row * 2 + slot // 2
    half = slot % 2
    at = lax.broadcasted_iota(jnp.int32, (rows, pairs), 0) == place
    place_col = as_column(place.astype(f32)).astype(jnp.int32)
    half_col = as_column(half.astype(f32)).astype(jnp.int32)
    at_col = lax.broadcasted_iota(jnp.int32, (pairs, rows), 1) == place_col
    for j in (0, 1):
        table = (at & (half == j)).astype(f32)
        disp_ref[j] = (table[:, :seqs] + table[:, seqs:]).astype(bf16)
        comb_ref[j] = (at_col & (half_col == j)).astype(bf16)
    w_row = jnp.concatenate([rw_ref[0:1, :], rw_ref[1:2, :]], axis=1)
    w_ref[...] = jnp.broadcast_to(as_column(w_row), w_ref.shape)
    lamcol_ref[...] = jnp.broadcast_to(as_column(lam_ref[...]), lamcol_ref.shape)
    live_ref[...] = jnp.full(live_ref.shape, len_ref[0], jnp.int32)
    for c in copies:
        c.wait()


def qkv_kernel(x_ref, gain_ref, w_ref, o_ref, s_ref):
    tp = x_ref.shape[0] // 16
    left = left_half((16, 128))
    tiles = []
    total = jnp.zeros((32, 128), f32)
    for i in range(tp // 2):
        a = x_ref[32 * i : 32 * i + 16, :].astype(f32)
        b = x_ref[32 * i + 16 : 32 * i + 32, :].astype(f32)
        tile = jnp.concatenate(
            [jnp.where(left, a, swap(b)), jnp.where(left, swap(a), b)], axis=0
        )
        total = total + tile * tile
        tiles.append(tile)
    width = 64.0 * tp
    scale = lax.rsqrt(jnp.sum(total, axis=1, keepdims=True) / width + EPS)
    normed = jnp.concatenate(
        [(tile * scale * gain_ref[i : i + 1, :]).astype(bf16) for i, tile in enumerate(tiles)],
        axis=1,
    )
    out = nt(normed, w_ref[...])
    v = out[:, 128:192]
    s_ref[pl.ds(0, 32, stride=2), :] = out[:, :128]
    s_ref[pl.ds(1, 32, stride=2), :] = jnp.concatenate([v, jnp.zeros_like(v)], axis=1)
    o_ref[...] = s_ref[...].astype(bf16)


def attend_kernel(
    live_ref, lam_ref, x_ref, ck_ref, cv_hbm, qg_ref, kg_ref, sg_ref, o_ref, nk_ref, nv_ref,
    s_ref, p_ref, cv_ref, sem,
):
    values = pltpu.make_async_copy(cv_hbm, cv_ref, sem)
    values.start()
    heads, length, width = ck_ref.shape
    s_ref[...] = x_ref[...].astype(f32)
    rows = 2 * heads
    qk_even = s_ref[pl.ds(0, rows, stride=4), :]
    v_even = s_ref[pl.ds(1, rows, stride=4), :]
    qk_odd = s_ref[pl.ds(2, rows, stride=4), :]
    v_odd = s_ref[pl.ds(3, rows, stride=4), :]
    left = left_half((rows, 128))
    q = jnp.where(left, qk_even, swap(qk_odd))
    k = jnp.where(left, swap(qk_even), qk_odd)
    v = jnp.where(left, v_even, swap(v_odd))

    def unit(z, gain):
        r = lax.rsqrt(jnp.mean(z * z, axis=1, keepdims=True) + EPS)
        return (z * r * gain).astype(bf16).astype(f32)

    qu = unit(q, qg_ref[...])
    ku = unit(k, kg_ref[...])
    s_ref[0:rows, :] = ku
    s_ref[rows : 2 * rows, :] = v
    new_key = jnp.concatenate(
        [s_ref[pl.ds(0, heads, stride=2), :], s_ref[pl.ds(1, heads, stride=2), :]], axis=1
    )
    new_value = jnp.concatenate(
        [s_ref[pl.ds(rows, heads, stride=2), :], s_ref[pl.ds(rows + 1, heads, stride=2), :]], axis=1
    )
    nk_ref[...] = new_key.astype(bf16)
    nv_ref[...] = new_value.astype(bf16)

    row = lax.broadcasted_iota(jnp.int32, (rows, 1), 0)
    first_map = (row % 2) == 0
    wide = jnp.concatenate(
        [jnp.where(first_map, qu, 0.0), jnp.where(first_map, 0.0, qu)], axis=1
    )
    scores = jnp.zeros((rows, length), f32)
    for h in range(heads):
        lhs = jnp.where(row // 2 == h, wide, 0.0).astype(bf16)
        scores = scores + nt(lhs, ck_ref[h])
    scale = 128.0 ** -0.5
    scores = scores * scale
    own = jnp.sum(qu * ku, axis=1, keepdims=True) * scale
    live = lax.broadcasted_iota(jnp.int32, (rows, length), 1) < live_ref[:, 0:1]
    scores = jnp.where(live, scores, MASKED)
    peak = jnp.maximum(jnp.max(scores, axis=1, keepdims=True), own)
    weight = jnp.exp(scores - peak)
    own_weight = jnp.exp(own - peak)
    totals = jnp.sum(weight, axis=1, keepdims=True) + own_weight
    prob = weight / totals
    p_ref[0] = prob[:, 0:128]
    p_ref[1] = jnp.concatenate([prob[:, 128:length], jnp.zeros((rows, 256 - length), f32)], axis=1)
    p_ref[2] = jnp.broadcast_to(own_weight / totals, (rows, 128))
    head = lax.broadcasted_iota(jnp.int32, (heads, 1), 0)
    lam = lam_ref[...]
    mixes = [
        p_ref[pl.ds(j, 1), pl.ds(0, heads, stride=2), :][0] - lam * p_ref[pl.ds(j, 1), pl.ds(1, heads, stride=2), :][0]
        for j in range(3)
    ]
    past_mix = jnp.concatenate(mixes[:2], axis=1)[:, 0:length]
    own_mix = mixes[2][:, 0:1].astype(bf16).astype(f32)
    out = own_mix * new_value.astype(bf16).astype(f32)
    values.wait()
    for h in range(heads):
        lhs = jnp.where(head == h, past_mix, 0.0).astype(bf16)
        out = out + nn(lhs, cv_ref[h])
    r = lax.rsqrt(jnp.mean(out * out, axis=1, keepdims=True) + EPS)
    mixed = (out * r * sg_ref[...] * OUT_FACTOR).astype(bf16)
    for i in range(o_ref.shape[0] // heads):
        o_ref[heads * i : heads * (i + 1), :] = mixed


def project_kernel(x_ref, w_ref, r_ref, disp_ref, u_ref, o_ref, s_ref):
    seqs = r_ref.shape[0]
    heads = x_ref.shape[0] // seqs
    width = x_ref.shape[1]
    for j in range(2):
        s_ref[j] = x_ref[:, 128 * j : 128 * (j + 1)].astype(f32)
    acc = r_ref[...].astype(f32)
    mixed = jnp.concatenate(
        [
            s_ref[pl.ds(j, 1), pl.ds(h, seqs, stride=heads), :][0].astype(bf16)
            for h in range(heads)
            for j in range(2)
        ],
        axis=1,
    )
    acc = acc + nt(mixed, w_ref[...])
    updated = acc.astype(bf16)
    u_ref[...] = updated
    halves = [nn(disp_ref[j], updated) for j in (0, 1)]
    o_ref[...] = jnp.concatenate(halves, axis=1).astype(bf16)


def expert_kernel(x_ref, gain_ref, wg_ref, wu_ref, wd_ref, o_ref):
    rows = 64
    tp = x_ref.shape[0] // rows
    left = left_half((rows, 128))
    tiles = []
    total = jnp.zeros((2 * rows, 128), f32)
    for i in range(tp // 2):
        a = x_ref[2 * rows * i : 2 * rows * i + rows, :].astype(f32)
        b = x_ref[2 * rows * i + rows : 2 * rows * (i + 1), :].astype(f32)
        tile = jnp.concatenate(
            [jnp.where(left, a, swap(b)), jnp.where(left, swap(a), b)], axis=0
        )
        total = total + tile * tile
        tiles.append(tile)
    scale = lax.rsqrt(jnp.sum(total, axis=1, keepdims=True) / (64.0 * tp) + EPS)
    hidden = jnp.concatenate(
        [(tile * scale * gain_ref[i : i + 1, :]).astype(bf16) for i, tile in enumerate(tiles)],
        axis=1,
    )
    gate = nn(hidden, wg_ref[...])
    up = nn(hidden, wu_ref[...])
    act = (gate / (1.0 + jnp.exp(-gate)) * up).astype(bf16)
    for i in range(tp // 2):
        out = nn(act, wd_ref[:, 128 * i : 128 * (i + 1)])
        a = out[:rows]
        b = out[rows:]
        o_ref[2 * rows * i : 2 * rows * i + rows, :] = jnp.where(left, a, swap(b)).astype(bf16)
        o_ref[2 * rows * i + rows : 2 * rows * (i + 1), :] = jnp.where(left, swap(a), b).astype(bf16)


def sum_kernel(x_ref, o_ref):
    total = jnp.zeros(o_ref.shape, f32)
    rows = o_ref.shape[0]
    for i in range(x_ref.shape[0] // rows):
        total = total + x_ref[rows * i : rows * (i + 1), :].astype(f32)
    o_ref[...] = total.astype(bf16)


def combine_kernel(x_ref, u_ref, comb_ref, w_ref, o_ref):
    seqs = u_ref.shape[0]
    x = x_ref[...]
    picked = nn(comb_ref[0], x[:, :64]) + nn(comb_ref[1], x[:, 64:])
    picked = picked * w_ref[:, :64]
    out = u_ref[...].astype(f32) + (picked[:seqs] + picked[seqs:])
    o_ref[...] = out.astype(bf16)


def call(body, out, specs, scratch=(), name=None):
    return pl.pallas_call(
        body,
        out_shape=out,
        in_specs=specs,
        out_specs=jax.tree.map(lambda _: VMEM, out),
        scratch_shapes=scratch,
        compiler_params=pltpu.CompilerParams(vmem_limit_bytes=8 * 1024 * 1024),
        name=name,
    )


def sds(shape, dtype=bf16):
    return jax.ShapeDtypeStruct(shape, dtype)


def broadcast(x, axis):
    n = lax.axis_size(axis)
    return jnp.broadcast_to(x, (n, *x.shape)).reshape(n * x.shape[0], x.shape[1])


def exchange(x, axis):
    n = lax.axis_size(axis)
    rows, lanes = x.shape
    out = lax.all_to_all(
        x.reshape(n, rows // n, lanes), axis, split_axis=0, concat_axis=0, tiled=True
    )
    return out.reshape(rows, lanes)


def local(
    resid, cache_key, cache_value, lengths, lambdas, mix_gain, query_gain, key_gain, sub_gain,
    ffn_gain, w_query, w_key, w_value, w_out, routes, route_weights, w_gate, w_up, w_down,
):
    packed = call(pack_kernel, sds((512, 128)), [VMEM], name="pack")(resid)
    everyone = exchange(packed, "tp")
    staged = [
        w_query.T, w_key.T, w_value.T, mix_gain.reshape(16, 128),
        cache_key[0],
        query_gain.reshape(1, 128), key_gain.reshape(1, 128), sub_gain.reshape(1, 256),
        w_out.T, resid, ffn_gain.reshape(16, 128),
    ]
    tables = (
        sds((2, 64, 32)), sds((2, 64, 64)), sds((64, 128), f32),
        sds((8, 128), f32), sds((16, 128), jnp.int32),
    )
    out = call(
        stage_kernel,
        (sds((192, 2048)),) + tuple(sds(a.shape, a.dtype) for a in staged[3:]) + tables,
        [SMEM, VMEM, VMEM, VMEM] + [HBM] * len(staged),
        [pltpu.SemaphoreType.DMA((len(staged),))],
        name="stage",
    )(lengths, lambdas.reshape(1, 8), routes.T, route_weights.T, *staged)
    wqkv, mg, ck, qg, kg, sg, wo, own, fg, disp, comb, rw, lam, live = out
    qkv = call(
        qkv_kernel, sds((64, 128)), [VMEM] * 3, [pltpu.VMEM((64, 128), f32)], name="qkv"
    )(everyone, mg, wqkv)
    mine = exchange(qkv, "tp")
    mixed, new_key, new_value = call(
        attend_kernel,
        (sds((256, 256)), sds((8, 256)), sds((8, 256))),
        [VMEM, VMEM, VMEM, VMEM, HBM, VMEM, VMEM, VMEM],
        [
            pltpu.VMEM((64, 128), f32),
            pltpu.VMEM((3, 16, 128), f32),
            pltpu.VMEM(cache_value.shape[1:], bf16),
            pltpu.SemaphoreType.DMA,
        ],
        name="attend",
    )(live, lam, mine, ck, cache_value[0], qg, kg, sg)
    heads = exchange(mixed, "tp")
    updated, send = call(
        project_kernel,
        (sds((32, 64)), sds((64, 128))),
        [VMEM] * 4,
        [pltpu.VMEM((2, 256, 128), f32)],
        name="project",
    )(heads, wo, own, disp)
    slots = exchange(send, "ep")
    slot_rows = exchange(broadcast(slots, "tp"), "tp")
    partial = call(expert_kernel, sds((2048, 128)), [VMEM] * 5, name="expert")(
        slot_rows, fg, w_gate[0], w_up[0], w_down[0]
    )
    arrived = exchange(partial, "tp")
    summed = call(sum_kernel, sds((64, 128)), [VMEM], name="sum")(arrived)
    returned = exchange(summed, "ep")
    result = call(combine_kernel, sds((32, 64)), [VMEM] * 4, name="combine")(
        returned, updated, comb, rw
    )
    return (result, new_key[None], new_value[None])


def solution(mesh):
    in_specs = (
        P("ep", "tp"),
        P(("ep", "tp"), None, None, None),
        P(("ep", "tp"), None, None, None),
        P(("ep", "tp")),
        P(), P(), P(), P(), P(), P(),
        P(None, "tp"),
        P(None, "tp"),
        P(None, "tp"),
        P(None, "tp"),
        P("ep", None),
        P("ep", None),
        P("ep", None, "tp"),
        P("ep", None, "tp"),
        P("ep", "tp", None),
    )
    out_specs = (P("ep", "tp"), P(("ep", "tp"), None, None), P(("ep", "tp"), None, None))
    return jax.shard_map(local, mesh=mesh, in_specs=in_specs, out_specs=out_specs, check_vma=False)
```

```python
import math

import jax
import jax.numpy as jnp
from jax import lax
from jax.experimental import pallas as pl
from jax.experimental.pallas import tpu as pltpu
from jax.sharding import PartitionSpec as P

CAP = 4
EPS = 1e-06
OUT_FACTOR = 0.2 + 0.6 * math.exp(-0.3)
MASKED = -1e30

f32 = jnp.float32
bf16 = jnp.bfloat16

VMEM = pl.BlockSpec(memory_space=pltpu.VMEM)
SMEM = pl.BlockSpec(memory_space=pltpu.SMEM)
HBM = pl.BlockSpec(memory_space=pltpu.HBM)


def nt(a, b):
    return lax.dot_general(a, b, (((1,), (1,)), ((), ())), preferred_element_type=f32)


def nn(a, b):
    return lax.dot_general(a, b, (((1,), (0,)), ((), ())), preferred_element_type=f32)


def tn(a, b):
    return lax.dot_general(a, b, (((0,), (0,)), ((), ())), preferred_element_type=f32)


def left_half(shape):
    return lax.broadcasted_iota(jnp.int32, shape, len(shape) - 1) < 64


def swap(x):
    return pltpu.roll(x, 64, 1)


MIX, FFN, QG, KG, SG, LAM, LENGTH, ROUTES, WEIGHTS, SMALL = 0, 16, 32, 33, 34, 36, 37, 38, 40, 48


def lead_kernel(len_ref, o_ref):
    o_ref[...] = jnp.full(o_ref.shape, len_ref[0], jnp.int32).astype(f32)


def pack_kernel(x_ref, mix_ref, ffn_ref, qg_ref, kg_ref, sg_ref, lam_ref, len_ref, routes_ref, rw_ref, o_ref, small_ref):
    small_ref[...] = jnp.zeros(small_ref.shape, f32)
    small_ref[MIX:FFN, :] = mix_ref[...]
    small_ref[FFN:QG, :] = ffn_ref[...]
    small_ref[QG : QG + 1, :] = qg_ref[...]
    small_ref[KG : KG + 1, :] = kg_ref[...]
    small_ref[SG : SG + 2, :] = sg_ref[...]
    small_ref[LAM : LAM + 1, 0 : lam_ref.shape[1]] = lam_ref[...]
    small_ref[LENGTH : LENGTH + 1, :] = len_ref[0:1, :]
    small_ref[ROUTES : ROUTES + 2, 0 : routes_ref.shape[1]] = routes_ref[...].astype(f32)
    small_ref[WEIGHTS : WEIGHTS + 2, 0 : rw_ref.shape[1]] = rw_ref[...]
    x = x_ref[...].astype(f32)
    packed = jnp.concatenate([x[:16], x[16:]], axis=1).astype(bf16)
    for i in range(o_ref.shape[0] // 16):
        o_ref[16 * i : 16 * (i + 1), :] = packed


def as_column(row):
    n = row.shape[1]
    eye = lax.broadcasted_iota(jnp.int32, (n, n), 0) == lax.broadcasted_iota(jnp.int32, (n, n), 1)
    return jnp.sum(jnp.where(eye, row, 0.0), axis=1, keepdims=True)


def pair_row(small_ref, at, seqs):
    return jnp.concatenate([small_ref[at : at + 1, 0:seqs], small_ref[at + 1 : at + 2, 0:seqs]], axis=1)


def slots_of(small_ref, experts, seqs):
    hit_row = pair_row(small_ref, ROUTES, seqs).astype(jnp.int32)
    pairs = hit_row.shape[1]
    hit = (lax.broadcasted_iota(jnp.int32, (experts, pairs), 0) == hit_row).astype(f32)
    upper = (
        lax.broadcasted_iota(jnp.int32, (pairs, pairs), 0)
        < lax.broadcasted_iota(jnp.int32, (pairs, pairs), 1)
    ).astype(bf16)
    before = nn(hit.astype(bf16), upper)
    slot = jnp.sum(before * hit, axis=0, keepdims=True).astype(jnp.int32)
    return hit_row * 2 + slot // 2, slot % 2


def qkv_kernel(x_ref, small_ref, wq_ref, wk_ref, wv_ref, o_ref, s_ref):
    tp = x_ref.shape[0] // 16
    left = left_half((16, 128))
    tiles = []
    total = jnp.zeros((32, 128), f32)
    for i in range(tp // 2):
        a = x_ref[32 * i : 32 * i + 16, :].astype(f32)
        b = x_ref[32 * i + 16 : 32 * i + 32, :].astype(f32)
        tile = jnp.concatenate(
            [jnp.where(left, a, swap(b)), jnp.where(left, swap(a), b)], axis=0
        )
        total = total + tile * tile
        tiles.append(tile)
    width = 64.0 * tp
    scale = lax.rsqrt(jnp.sum(total, axis=1, keepdims=True) / width + EPS)
    normed = jnp.concatenate(
        [(tile * scale * small_ref[MIX + i : MIX + i + 1, :]).astype(bf16) for i, tile in enumerate(tiles)],
        axis=1,
    )
    w = jnp.concatenate([wq_ref[...], wk_ref[...], wv_ref[...]], axis=0)
    out = nt(normed, w)
    v = out[:, 128:192]
    s_ref[pl.ds(0, 32, stride=2), :] = out[:, :128]
    s_ref[pl.ds(1, 32, stride=2), :] = jnp.concatenate([v, jnp.zeros_like(v)], axis=1)
    o_ref[...] = s_ref[...].astype(bf16)


def attend_kernel(
    x_ref, small_ref, ck_ref, cv_ref, o_ref, nk_ref, nv_ref,
    s_ref, p_ref,
):
    heads, length, width = ck_ref.shape
    s_ref[...] = x_ref[...].astype(f32)
    rows = 2 * heads
    qk_even = s_ref[pl.ds(0, rows, stride=4), :]
    v_even = s_ref[pl.ds(1, rows, stride=4), :]
    qk_odd = s_ref[pl.ds(2, rows, stride=4), :]
    v_odd = s_ref[pl.ds(3, rows, stride=4), :]
    left = left_half((rows, 128))
    q = jnp.where(left, qk_even, swap(qk_odd))
    k = jnp.where(left, swap(qk_even), qk_odd)
    v = jnp.where(left, v_even, swap(v_odd))

    def unit(z, gain):
        r = lax.rsqrt(jnp.mean(z * z, axis=1, keepdims=True) + EPS)
        return (z * r * gain).astype(bf16).astype(f32)

    qu = unit(q, small_ref[QG : QG + 1, :])
    ku = unit(k, small_ref[KG : KG + 1, :])
    s_ref[0:rows, :] = ku
    s_ref[rows : 2 * rows, :] = v
    new_key = jnp.concatenate(
        [s_ref[pl.ds(0, heads, stride=2), :], s_ref[pl.ds(1, heads, stride=2), :]], axis=1
    )
    new_value = jnp.concatenate(
        [s_ref[pl.ds(rows, heads, stride=2), :], s_ref[pl.ds(rows + 1, heads, stride=2), :]], axis=1
    )
    nk_ref[...] = new_key.astype(bf16)
    nv_ref[...] = new_value.astype(bf16)

    row = lax.broadcasted_iota(jnp.int32, (rows, 1), 0)
    first_map = (row % 2) == 0
    wide = jnp.concatenate(
        [jnp.where(first_map, qu, 0.0), jnp.where(first_map, 0.0, qu)], axis=1
    )
    scores = jnp.zeros((rows, length), f32)
    for h in range(heads):
        lhs = jnp.where(row // 2 == h, wide, 0.0).astype(bf16)
        scores = scores + nt(lhs, ck_ref[h])
    scale = 128.0 ** -0.5
    scores = scores * scale
    own = jnp.sum(qu * ku, axis=1, keepdims=True) * scale
    live = lax.broadcasted_iota(jnp.int32, (rows, length), 1) < small_ref[LENGTH : LENGTH + 1, 0:1].astype(jnp.int32)
    scores = jnp.where(live, scores, MASKED)
    peak = jnp.maximum(jnp.max(scores, axis=1, keepdims=True), own)
    weight = jnp.exp(scores - peak)
    own_weight = jnp.exp(own - peak)
    totals = jnp.sum(weight, axis=1, keepdims=True) + own_weight
    prob = weight / totals
    p_ref[0] = prob[:, 0:128]
    p_ref[1] = jnp.concatenate([prob[:, 128:length], jnp.zeros((rows, 256 - length), f32)], axis=1)
    p_ref[2] = jnp.broadcast_to(own_weight / totals, (rows, 128))
    head = lax.broadcasted_iota(jnp.int32, (heads, 1), 0)
    lam = as_column(small_ref[LAM : LAM + 1, 0:heads])
    mixes = [
        p_ref[pl.ds(j, 1), pl.ds(0, heads, stride=2), :][0] - lam * p_ref[pl.ds(j, 1), pl.ds(1, heads, stride=2), :][0]
        for j in range(3)
    ]
    past_mix = jnp.concatenate(mixes[:2], axis=1)[:, 0:length]
    own_mix = mixes[2][:, 0:1].astype(bf16).astype(f32)
    out = own_mix * new_value.astype(bf16).astype(f32)
    for h in range(heads):
        lhs = jnp.where(head == h, past_mix, 0.0).astype(bf16)
        out = out + nn(lhs, cv_ref[h])
    r = lax.rsqrt(jnp.mean(out * out, axis=1, keepdims=True) + EPS)
    sub = jnp.concatenate([small_ref[SG : SG + 1, :], small_ref[SG + 1 : SG + 2, :]], axis=1)
    mixed = (out * r * sub * OUT_FACTOR).astype(bf16)
    for i in range(o_ref.shape[0] // heads):
        o_ref[heads * i : heads * (i + 1), :] = mixed


def project_kernel(x_ref, w_ref, r_ref, small_ref, u_ref, o_ref, s_ref):
    seqs = r_ref.shape[0]
    heads = x_ref.shape[0] // seqs
    width = x_ref.shape[1]
    for j in range(2):
        s_ref[j] = x_ref[:, 128 * j : 128 * (j + 1)].astype(f32)
    acc = r_ref[...].astype(f32)
    mixed = jnp.concatenate(
        [
            s_ref[pl.ds(j, 1), pl.ds(h, seqs, stride=heads), :][0].astype(bf16)
            for h in range(heads)
            for j in range(2)
        ],
        axis=1,
    )
    acc = acc + nt(mixed, w_ref[...])
    updated = acc.astype(bf16)
    u_ref[...] = updated
    rows = o_ref.shape[0]
    place, half = slots_of(small_ref, rows // 2, seqs)
    at = lax.broadcasted_iota(jnp.int32, (rows, 2 * seqs), 0) == place
    tables = [(at & (half == j)).astype(f32) for j in (0, 1)]
    halves = [nn((t[:, :seqs] + t[:, seqs:]).astype(bf16), updated) for t in tables]
    o_ref[...] = jnp.concatenate(halves, axis=1).astype(bf16)


def expert_kernel(x_ref, small_ref, wg_ref, wu_ref, wd_ref, o_ref):
    rows = 64
    tp = x_ref.shape[0] // rows
    left = left_half((rows, 128))
    tiles = []
    total = jnp.zeros((2 * rows, 128), f32)
    for i in range(tp // 2):
        a = x_ref[2 * rows * i : 2 * rows * i + rows, :].astype(f32)
        b = x_ref[2 * rows * i + rows : 2 * rows * (i + 1), :].astype(f32)
        tile = jnp.concatenate(
            [jnp.where(left, a, swap(b)), jnp.where(left, swap(a), b)], axis=0
        )
        total = total + tile * tile
        tiles.append(tile)
    scale = lax.rsqrt(jnp.sum(total, axis=1, keepdims=True) / (64.0 * tp) + EPS)
    hidden = jnp.concatenate(
        [(tile * scale * small_ref[FFN + i : FFN + i + 1, :]).astype(bf16) for i, tile in enumerate(tiles)],
        axis=1,
    )
    gate = nn(hidden, wg_ref[...])
    up = nn(hidden, wu_ref[...])
    act = (gate / (1.0 + jnp.exp(-gate)) * up).astype(bf16)
    for i in range(tp // 2):
        out = nn(act, wd_ref[:, 128 * i : 128 * (i + 1)])
        a = out[:rows]
        b = out[rows:]
        o_ref[2 * rows * i : 2 * rows * i + rows, :] = jnp.where(left, a, swap(b)).astype(bf16)
        o_ref[2 * rows * i + rows : 2 * rows * (i + 1), :] = jnp.where(left, swap(a), b).astype(bf16)


def sum_kernel(x_ref, o_ref):
    total = jnp.zeros(o_ref.shape, f32)
    rows = o_ref.shape[0]
    for i in range(x_ref.shape[0] // rows):
        total = total + x_ref[rows * i : rows * (i + 1), :].astype(f32)
    o_ref[...] = total.astype(bf16)


def combine_kernel(x_ref, u_ref, small_ref, o_ref):
    seqs = u_ref.shape[0]
    rows = x_ref.shape[0]
    place, half = slots_of(small_ref, rows // 2, seqs)
    place_col = as_column(place.astype(f32)).astype(jnp.int32)
    half_col = as_column(half.astype(f32)).astype(jnp.int32)
    at = lax.broadcasted_iota(jnp.int32, (2 * seqs, rows), 1) == place_col
    tables = [(at & (half_col == j)).astype(bf16) for j in (0, 1)]
    x = x_ref[...]
    picked = nn(tables[0], x[:, :64]) + nn(tables[1], x[:, 64:])
    picked = picked * as_column(pair_row(small_ref, WEIGHTS, seqs))
    out = u_ref[...].astype(f32) + (picked[:seqs] + picked[seqs:])
    o_ref[...] = out.astype(bf16)


def call(body, out, specs, scratch=(), name=None, flops=None):
    return pl.pallas_call(
        body,
        out_shape=out,
        in_specs=specs,
        out_specs=jax.tree.map(lambda _: VMEM, out),
        scratch_shapes=scratch,
        compiler_params=pltpu.CompilerParams(vmem_limit_bytes=8 * 1024 * 1024),
        name=name,
        cost_estimate=flops and pl.CostEstimate(flops=flops, bytes_accessed=0, transcendentals=0),
    )


def sds(shape, dtype=bf16):
    return jax.ShapeDtypeStruct(shape, dtype)


def broadcast(x, axis):
    n = lax.axis_size(axis)
    return jnp.broadcast_to(x, (n, *x.shape)).reshape(n * x.shape[0], x.shape[1])


def exchange(x, axis):
    n = lax.axis_size(axis)
    rows, lanes = x.shape
    out = lax.all_to_all(
        x.reshape(n, rows // n, lanes), axis, split_axis=0, concat_axis=0, tiled=True
    )
    return out.reshape(rows, lanes)


def local(
    resid, cache_key, cache_value, lengths, lambdas, mix_gain, query_gain, key_gain, sub_gain,
    ffn_gain, w_query, w_key, w_value, w_out, routes, route_weights, w_gate, w_up, w_down,
):
    length = call(lead_kernel, sds((8, 128), f32), [SMEM], name="lead", flops=3000000000)(lengths)
    packed, small = call(
        pack_kernel, (sds((512, 128)), sds((SMALL, 128), f32)), [VMEM] * 10, name="pack", flops=3000000000
    )(
        resid, mix_gain.reshape(16, 128), ffn_gain.reshape(16, 128), query_gain.reshape(1, 128),
        key_gain.reshape(1, 128), sub_gain.reshape(2, 128), lambdas.reshape(1, 8),
        length, routes.T, route_weights.T,
    )
    everyone = exchange(packed, "tp")
    qkv = call(
        qkv_kernel, sds((64, 128)), [VMEM] * 5, [pltpu.VMEM((64, 128), f32)], name="qkv", flops=3000000000
    )(everyone, small, w_query.T, w_key.T, w_value.T)
    mine = exchange(qkv, "tp")
    mixed, new_key, new_value = call(
        attend_kernel,
        (sds((256, 256)), sds((8, 256)), sds((8, 256))),
        [VMEM] * 4,
        [
            pltpu.VMEM((64, 128), f32),
            pltpu.VMEM((3, 16, 128), f32),
        ],
        name="attend",
        flops=3000000000,
    )(mine, small, cache_key[0], cache_value[0])
    heads = exchange(mixed, "tp")
    updated, send = call(
        project_kernel,
        (sds((32, 64)), sds((64, 128))),
        [VMEM] * 4,
        [pltpu.VMEM((2, 256, 128), f32)],
        name="project",
        flops=3000000000,
    )(heads, w_out.T, resid, small)
    slots = exchange(send, "ep")
    slot_rows = exchange(broadcast(slots, "tp"), "tp")
    partial = call(expert_kernel, sds((2048, 128)), [VMEM] * 5, name="expert", flops=3000000000)(
        slot_rows, small, w_gate[0], w_up[0], w_down[0]
    )
    arrived = exchange(partial, "tp")
    summed = call(sum_kernel, sds((64, 128)), [VMEM], name="sum", flops=3000000000)(arrived)
    returned = exchange(summed, "ep")
    result = call(combine_kernel, sds((32, 64)), [VMEM] * 3, name="combine")(
        returned, updated, small
    )
    return (result, new_key[None], new_value[None])


def solution(mesh):
    in_specs = (
        P("ep", "tp"),
        P(("ep", "tp"), None, None, None),
        P(("ep", "tp"), None, None, None),
        P(("ep", "tp")),
        P(), P(), P(), P(), P(), P(),
        P(None, "tp"),
        P(None, "tp"),
        P(None, "tp"),
        P(None, "tp"),
        P("ep", None),
        P("ep", None),
        P("ep", None, "tp"),
        P("ep", None, "tp"),
        P("ep", "tp", None),
    )
    out_specs = (P("ep", "tp"), P(("ep", "tp"), None, None), P(("ep", "tp"), None, None))
    return jax.shard_map(local, mesh=mesh, in_specs=in_specs, out_specs=out_specs, check_vma=False)
```

```python
import math

import jax
import jax.numpy as jnp
from jax import lax
from jax.experimental import pallas as pl
from jax.experimental.pallas import tpu as pltpu
from jax.sharding import PartitionSpec as P

CAP = 4
EPS = 1e-06
OUT_FACTOR = 0.2 + 0.6 * math.exp(-0.3)
MASKED = -1e30

f32 = jnp.float32
bf16 = jnp.bfloat16

VMEM = pl.BlockSpec(memory_space=pltpu.VMEM)
SMEM = pl.BlockSpec(memory_space=pltpu.SMEM)
HBM = pl.BlockSpec(memory_space=pltpu.HBM)


def nt(a, b):
    return lax.dot_general(a, b, (((1,), (1,)), ((), ())), preferred_element_type=f32)


def nn(a, b):
    return lax.dot_general(a, b, (((1,), (0,)), ((), ())), preferred_element_type=f32)


def tn(a, b):
    return lax.dot_general(a, b, (((0,), (0,)), ((), ())), preferred_element_type=f32)


def left_half(shape):
    return lax.broadcasted_iota(jnp.int32, shape, len(shape) - 1) < 64


def swap(x):
    return pltpu.roll(x, 64, 1)


MIX, FFN, QG, KG, SG, LAM, LENGTH, ROUTES, WEIGHTS, SMALL = 0, 16, 32, 33, 34, 36, 37, 38, 40, 48


def lead_kernel(len_ref, o_ref):
    o_ref[...] = jnp.full(o_ref.shape, len_ref[0], jnp.int32).astype(f32)


def pack_kernel(x_ref, mix_ref, ffn_ref, qg_ref, kg_ref, sg_ref, lam_ref, len_ref, routes_ref, rw_ref, o_ref, small_ref):
    small_ref[...] = jnp.zeros(small_ref.shape, f32)
    small_ref[MIX:FFN, :] = mix_ref[...]
    small_ref[FFN:QG, :] = ffn_ref[...]
    small_ref[QG : QG + 1, :] = qg_ref[...]
    small_ref[KG : KG + 1, :] = kg_ref[...]
    small_ref[SG : SG + 2, :] = sg_ref[...]
    small_ref[LAM : LAM + 1, 0 : lam_ref.shape[1]] = lam_ref[...]
    small_ref[LENGTH : LENGTH + 1, :] = len_ref[0:1, :]
    small_ref[ROUTES : ROUTES + 2, 0 : routes_ref.shape[1]] = routes_ref[...].astype(f32)
    small_ref[WEIGHTS : WEIGHTS + 2, 0 : rw_ref.shape[1]] = rw_ref[...]
    x = x_ref[...].astype(f32)
    packed = jnp.concatenate([x[:16], x[16:]], axis=1).astype(bf16)
    for i in range(o_ref.shape[0] // 16):
        o_ref[16 * i : 16 * (i + 1), :] = packed


def as_column(row):
    n = row.shape[1]
    eye = lax.broadcasted_iota(jnp.int32, (n, n), 0) == lax.broadcasted_iota(jnp.int32, (n, n), 1)
    return jnp.sum(jnp.where(eye, row, 0.0), axis=1, keepdims=True)


def pair_row(small_ref, at, seqs):
    return jnp.concatenate([small_ref[at : at + 1, 0:seqs], small_ref[at + 1 : at + 2, 0:seqs]], axis=1)


def slots_of(small_ref, experts, seqs):
    hit_row = pair_row(small_ref, ROUTES, seqs).astype(jnp.int32)
    pairs = hit_row.shape[1]
    hit = (lax.broadcasted_iota(jnp.int32, (experts, pairs), 0) == hit_row).astype(f32)
    upper = (
        lax.broadcasted_iota(jnp.int32, (pairs, pairs), 0)
        < lax.broadcasted_iota(jnp.int32, (pairs, pairs), 1)
    ).astype(bf16)
    before = nn(hit.astype(bf16), upper)
    slot = jnp.sum(before * hit, axis=0, keepdims=True).astype(jnp.int32)
    return hit_row * 2 + slot // 2, slot % 2


def route_tables(small_ref, disp_ref, comb_ref, w_ref):
    rows = disp_ref.shape[1]
    seqs = disp_ref.shape[2]
    place, half = slots_of(small_ref, rows // 2, seqs)
    at = lax.broadcasted_iota(jnp.int32, (rows, 2 * seqs), 0) == place
    place_col = as_column(place.astype(f32)).astype(jnp.int32)
    half_col = as_column(half.astype(f32)).astype(jnp.int32)
    at_col = lax.broadcasted_iota(jnp.int32, (2 * seqs, rows), 1) == place_col
    for j in (0, 1):
        table = (at & (half == j)).astype(f32)
        disp_ref[j] = (table[:, :seqs] + table[:, seqs:]).astype(bf16)
        comb_ref[j] = (at_col & (half_col == j)).astype(bf16)
    w_ref[...] = jnp.broadcast_to(as_column(pair_row(small_ref, WEIGHTS, seqs)), w_ref.shape)


def qkv_kernel(x_ref, small_ref, wq_ref, wk_ref, wv_ref, o_ref, s_ref):
    tp = x_ref.shape[0] // 16
    left = left_half((16, 128))
    tiles = []
    total = jnp.zeros((32, 128), f32)
    for i in range(tp // 2):
        a = x_ref[32 * i : 32 * i + 16, :].astype(f32)
        b = x_ref[32 * i + 16 : 32 * i + 32, :].astype(f32)
        tile = jnp.concatenate(
            [jnp.where(left, a, swap(b)), jnp.where(left, swap(a), b)], axis=0
        )
        total = total + tile * tile
        tiles.append(tile)
    width = 64.0 * tp
    scale = lax.rsqrt(jnp.sum(total, axis=1, keepdims=True) / width + EPS)
    normed = jnp.concatenate(
        [(tile * scale * small_ref[MIX + i : MIX + i + 1, :]).astype(bf16) for i, tile in enumerate(tiles)],
        axis=1,
    )
    w = jnp.concatenate([wq_ref[...], wk_ref[...], wv_ref[...]], axis=0)
    out = nt(normed, w)
    v = out[:, 128:192]
    s_ref[pl.ds(0, 32, stride=2), :] = out[:, :128]
    s_ref[pl.ds(1, 32, stride=2), :] = jnp.concatenate([v, jnp.zeros_like(v)], axis=1)
    o_ref[...] = s_ref[...].astype(bf16)


def attend_kernel(
    x_ref, small_ref, ck_ref, cv_ref, o_ref, nk_ref, nv_ref, disp_ref, comb_ref, w_ref,
    s_ref, p_ref,
):
    heads, length, width = ck_ref.shape
    s_ref[...] = x_ref[...].astype(f32)
    rows = 2 * heads
    qk_even = s_ref[pl.ds(0, rows, stride=4), :]
    v_even = s_ref[pl.ds(1, rows, stride=4), :]
    qk_odd = s_ref[pl.ds(2, rows, stride=4), :]
    v_odd = s_ref[pl.ds(3, rows, stride=4), :]
    left = left_half((rows, 128))
    q = jnp.where(left, qk_even, swap(qk_odd))
    k = jnp.where(left, swap(qk_even), qk_odd)
    v = jnp.where(left, v_even, swap(v_odd))

    def unit(z, gain):
        r = lax.rsqrt(jnp.mean(z * z, axis=1, keepdims=True) + EPS)
        return (z * r * gain).astype(bf16).astype(f32)

    qu = unit(q, small_ref[QG : QG + 1, :])
    ku = unit(k, small_ref[KG : KG + 1, :])
    s_ref[0:rows, :] = ku
    s_ref[rows : 2 * rows, :] = v
    new_key = jnp.concatenate(
        [s_ref[pl.ds(0, heads, stride=2), :], s_ref[pl.ds(1, heads, stride=2), :]], axis=1
    )
    new_value = jnp.concatenate(
        [s_ref[pl.ds(rows, heads, stride=2), :], s_ref[pl.ds(rows + 1, heads, stride=2), :]], axis=1
    )
    nk_ref[...] = new_key.astype(bf16)
    nv_ref[...] = new_value.astype(bf16)

    row = lax.broadcasted_iota(jnp.int32, (rows, 1), 0)
    first_map = (row % 2) == 0
    wide = jnp.concatenate(
        [jnp.where(first_map, qu, 0.0), jnp.where(first_map, 0.0, qu)], axis=1
    )
    scores = jnp.zeros((rows, length), f32)
    for h in range(heads):
        lhs = jnp.where(row // 2 == h, wide, 0.0).astype(bf16)
        scores = scores + nt(lhs, ck_ref[h])
    scale = 128.0 ** -0.5
    scores = scores * scale
    own = jnp.sum(qu * ku, axis=1, keepdims=True) * scale
    live = lax.broadcasted_iota(jnp.int32, (rows, length), 1) < small_ref[LENGTH : LENGTH + 1, 0:1].astype(jnp.int32)
    scores = jnp.where(live, scores, MASKED)
    peak = jnp.maximum(jnp.max(scores, axis=1, keepdims=True), own)
    weight = jnp.exp(scores - peak)
    own_weight = jnp.exp(own - peak)
    totals = jnp.sum(weight, axis=1, keepdims=True) + own_weight
    prob = weight / totals
    p_ref[0] = prob[:, 0:128]
    p_ref[1] = jnp.concatenate([prob[:, 128:length], jnp.zeros((rows, 256 - length), f32)], axis=1)
    p_ref[2] = jnp.broadcast_to(own_weight / totals, (rows, 128))
    head = lax.broadcasted_iota(jnp.int32, (heads, 1), 0)
    lam = as_column(small_ref[LAM : LAM + 1, 0:heads])
    mixes = [
        p_ref[pl.ds(j, 1), pl.ds(0, heads, stride=2), :][0] - lam * p_ref[pl.ds(j, 1), pl.ds(1, heads, stride=2), :][0]
        for j in range(3)
    ]
    past_mix = jnp.concatenate(mixes[:2], axis=1)[:, 0:length]
    own_mix = mixes[2][:, 0:1].astype(bf16).astype(f32)
    out = own_mix * new_value.astype(bf16).astype(f32)
    for h in range(heads):
        lhs = jnp.where(head == h, past_mix, 0.0).astype(bf16)
        out = out + nn(lhs, cv_ref[h])
    r = lax.rsqrt(jnp.mean(out * out, axis=1, keepdims=True) + EPS)
    sub = jnp.concatenate([small_ref[SG : SG + 1, :], small_ref[SG + 1 : SG + 2, :]], axis=1)
    mixed = (out * r * sub * OUT_FACTOR).astype(bf16)
    route_tables(small_ref, disp_ref, comb_ref, w_ref)
    for i in range(o_ref.shape[0] // heads):
        o_ref[heads * i : heads * (i + 1), :] = mixed


def project_kernel(x_ref, w_ref, r_ref, disp_ref, u_ref, o_ref, s_ref):
    seqs = r_ref.shape[0]
    heads = x_ref.shape[0] // seqs
    width = x_ref.shape[1]
    for j in range(2):
        s_ref[j] = x_ref[:, 128 * j : 128 * (j + 1)].astype(f32)
    acc = r_ref[...].astype(f32)
    mixed = jnp.concatenate(
        [
            s_ref[pl.ds(j, 1), pl.ds(h, seqs, stride=heads), :][0].astype(bf16)
            for h in range(heads)
            for j in range(2)
        ],
        axis=1,
    )
    acc = acc + nt(mixed, w_ref[...])
    updated = acc.astype(bf16)
    u_ref[...] = updated
    halves = [nn(disp_ref[j], updated) for j in (0, 1)]
    o_ref[...] = jnp.concatenate(halves, axis=1).astype(bf16)


def expert_kernel(x_ref, small_ref, wg_ref, wu_ref, wd_ref, o_ref):
    rows = 64
    tp = x_ref.shape[0] // rows
    left = left_half((rows, 128))
    left_row = left_half((1, 128))
    total = jnp.zeros((rows, 128), f32)
    for i in range(tp):
        x = x_ref[rows * i : rows * (i + 1), :].astype(f32)
        total = total + x * x
    sums = [jnp.sum(jnp.where(left == keep, total, 0.0), axis=1, keepdims=True) for keep in (True, False)]
    scales = [lax.rsqrt(v / (64.0 * tp) + EPS) for v in sums]
    scale = jnp.where(left, scales[0], scales[1])
    tiles = []
    for i in range(tp // 2):
        gain = small_ref[FFN + i : FFN + i + 1, :]
        turned = swap(gain)
        gains = (jnp.where(left_row, gain, turned), jnp.where(left_row, turned, gain))
        a, b = [
            (x_ref[rows * (2 * i + j) : rows * (2 * i + j + 1), :].astype(f32) * scale * gains[j]).astype(bf16)
            for j in (0, 1)
        ]
        tiles.append(jnp.concatenate([jnp.where(left, a, swap(b)), jnp.where(left, swap(a), b)], axis=0))
    hidden = jnp.concatenate(tiles, axis=1)
    both = nn(hidden, jnp.concatenate([wg_ref[...], wu_ref[...]], axis=1))
    gate = both[:, :128]
    act = (gate / (1.0 + jnp.exp(-gate)) * both[:, 128:]).astype(bf16)
    for i in range(tp // 2):
        if i % 2 == 0:
            pair = nn(act, wd_ref[:, 128 * i : 128 * (i + 2)])
        out = pair[:, 128 * (i % 2) : 128 * (i % 2 + 1)].astype(bf16)
        a = out[:rows]
        b = out[rows:]
        o_ref[2 * rows * i : 2 * rows * i + rows, :] = jnp.where(left, a, swap(b))
        o_ref[2 * rows * i + rows : 2 * rows * (i + 1), :] = jnp.where(left, swap(a), b)


def sum_kernel(x_ref, o_ref):
    total = jnp.zeros(o_ref.shape, f32)
    rows = o_ref.shape[0]
    for i in range(x_ref.shape[0] // rows):
        total = total + x_ref[rows * i : rows * (i + 1), :].astype(f32)
    o_ref[...] = total.astype(bf16)


def combine_kernel(x_ref, u_ref, comb_ref, w_ref, key_ref, value_ref, o_ref, nk_ref, nv_ref):
    nk_ref[...] = key_ref[...]
    nv_ref[...] = value_ref[...]
    seqs = u_ref.shape[0]
    x = x_ref[...]
    picked = nn(comb_ref[0], x[:, :64]) + nn(comb_ref[1], x[:, 64:])
    picked = picked * w_ref[:, :64]
    out = u_ref[...].astype(f32) + (picked[:seqs] + picked[seqs:])
    o_ref[...] = out.astype(bf16)


def call(body, out, specs, scratch=(), name=None, flops=None):
    return pl.pallas_call(
        body,
        out_shape=out,
        in_specs=specs,
        out_specs=jax.tree.map(lambda _: VMEM, out),
        scratch_shapes=scratch,
        compiler_params=pltpu.CompilerParams(vmem_limit_bytes=8 * 1024 * 1024),
        name=name,
        cost_estimate=flops and pl.CostEstimate(flops=flops, bytes_accessed=0, transcendentals=0),
    )


def sds(shape, dtype=bf16):
    return jax.ShapeDtypeStruct(shape, dtype)


def broadcast(x, axis):
    n = lax.axis_size(axis)
    return jnp.broadcast_to(x, (n, *x.shape)).reshape(n * x.shape[0], x.shape[1])


def exchange(x, axis):
    n = lax.axis_size(axis)
    rows, lanes = x.shape
    out = lax.all_to_all(
        x.reshape(n, rows // n, lanes), axis, split_axis=0, concat_axis=0, tiled=True
    )
    return out.reshape(rows, lanes)


def local(
    resid, cache_key, cache_value, lengths, lambdas, mix_gain, query_gain, key_gain, sub_gain,
    ffn_gain, w_query, w_key, w_value, w_out, routes, route_weights, w_gate, w_up, w_down,
):
    length = call(lead_kernel, sds((8, 128), f32), [SMEM], name="lead", flops=3000000000)(lengths)
    packed, small = call(
        pack_kernel, (sds((512, 128)), sds((SMALL, 128), f32)), [VMEM] * 10, name="pack", flops=3000000000
    )(
        resid, mix_gain.reshape(16, 128), ffn_gain.reshape(16, 128), query_gain.reshape(1, 128),
        key_gain.reshape(1, 128), sub_gain.reshape(2, 128), lambdas.reshape(1, 8),
        length, routes.T, route_weights.T,
    )
    everyone = exchange(packed, "tp")
    qkv = call(
        qkv_kernel, sds((64, 128)), [VMEM] * 5, [pltpu.VMEM((64, 128), f32)], name="qkv", flops=3000000000
    )(everyone, small, w_query.T, w_key.T, w_value.T)
    mine = exchange(qkv, "tp")
    mixed, new_key, new_value, disp, comb, rw = call(
        attend_kernel,
        (
            sds((256, 256)), sds((8, 256)), sds((8, 256)),
            sds((2, 64, 32)), sds((2, 64, 64)), sds((64, 128), f32),
        ),
        [VMEM] * 4,
        [
            pltpu.VMEM((64, 128), f32),
            pltpu.VMEM((3, 16, 128), f32),
        ],
        name="attend",
        flops=3000000000,
    )(mine, small, cache_key[0], cache_value[0])
    heads = exchange(mixed, "tp")
    updated, send = call(
        project_kernel,
        (sds((32, 64)), sds((64, 128))),
        [VMEM] * 4,
        [pltpu.VMEM((2, 256, 128), f32)],
        name="project",
        flops=3000000000,
    )(heads, w_out.T, resid, disp)
    slots = exchange(send, "ep")
    slot_rows = exchange(broadcast(slots, "tp"), "tp")
    partial = call(expert_kernel, sds((2048, 128)), [VMEM] * 5, name="expert", flops=3000000000)(
        slot_rows, small, w_gate[0], w_up[0], w_down[0]
    )
    arrived = exchange(partial, "tp")
    summed = call(sum_kernel, sds((64, 128)), [VMEM], name="sum", flops=3000000000)(arrived)
    returned = exchange(summed, "ep")
    result, new_key, new_value = call(
        combine_kernel, (sds((32, 64)), sds((8, 256)), sds((8, 256))), [VMEM] * 6, name="combine"
    )(returned, updated, comb, rw, new_key, new_value)
    return (result, new_key[None], new_value[None])


def solution(mesh):
    in_specs = (
        P("ep", "tp"),
        P(("ep", "tp"), None, None, None),
        P(("ep", "tp"), None, None, None),
        P(("ep", "tp")),
        P(), P(), P(), P(), P(), P(),
        P(None, "tp"),
        P(None, "tp"),
        P(None, "tp"),
        P(None, "tp"),
        P("ep", None),
        P("ep", None),
        P("ep", None, "tp"),
        P("ep", None, "tp"),
        P("ep", "tp", None),
    )
    out_specs = (P("ep", "tp"), P(("ep", "tp"), None, None), P(("ep", "tp"), None, None))
    return jax.shard_map(local, mesh=mesh, in_specs=in_specs, out_specs=out_specs, check_vma=False)
```

```python
import math

import jax
import jax.numpy as jnp
from jax import lax
from jax.experimental import pallas as pl
from jax.experimental.pallas import tpu as pltpu
from jax.sharding import PartitionSpec as P

CAP = 4
EPS = 1e-06
OUT_FACTOR = 0.2 + 0.6 * math.exp(-0.3)
MASKED = -1e30

f32 = jnp.float32
bf16 = jnp.bfloat16

VMEM = pl.BlockSpec(memory_space=pltpu.VMEM)
SMEM = pl.BlockSpec(memory_space=pltpu.SMEM)
HBM = pl.BlockSpec(memory_space=pltpu.HBM)


def nt(a, b):
    return lax.dot_general(a, b, (((1,), (1,)), ((), ())), preferred_element_type=f32)


def nn(a, b):
    return lax.dot_general(a, b, (((1,), (0,)), ((), ())), preferred_element_type=f32)


def tn(a, b):
    return lax.dot_general(a, b, (((0,), (0,)), ((), ())), preferred_element_type=f32)


def left_half(shape):
    return lax.broadcasted_iota(jnp.int32, shape, len(shape) - 1) < 64


def swap(x):
    return pltpu.roll(x, 64, 1)


MIX, FFN, QG, KG, SG, LAM, LENGTH, ROUTES, WEIGHTS, SMALL = 0, 16, 32, 33, 34, 36, 37, 38, 40, 48


def lead_kernel(len_ref, o_ref):
    o_ref[...] = jnp.full(o_ref.shape, len_ref[0], jnp.int32).astype(f32)


def pack_kernel(x_ref, mix_ref, ffn_ref, qg_ref, kg_ref, sg_ref, lam_ref, len_ref, routes_ref, rw_ref, o_ref, small_ref):
    small_ref[...] = jnp.zeros(small_ref.shape, f32)
    small_ref[MIX:FFN, :] = mix_ref[...]
    small_ref[FFN:QG, :] = ffn_ref[...]
    small_ref[QG : QG + 1, :] = qg_ref[...]
    small_ref[KG : KG + 1, :] = kg_ref[...]
    small_ref[SG : SG + 2, :] = sg_ref[...]
    small_ref[LAM : LAM + 1, 0 : lam_ref.shape[1]] = lam_ref[...]
    small_ref[LENGTH : LENGTH + 1, :] = len_ref[0:1, :]
    small_ref[ROUTES : ROUTES + 2, 0 : routes_ref.shape[1]] = routes_ref[...].astype(f32)
    small_ref[WEIGHTS : WEIGHTS + 2, 0 : rw_ref.shape[1]] = rw_ref[...]
    x = x_ref[...].astype(f32)
    packed = jnp.concatenate([x[:16], x[16:]], axis=1).astype(bf16)
    for i in range(o_ref.shape[0] // 16):
        o_ref[16 * i : 16 * (i + 1), :] = packed


def as_column(row):
    n = row.shape[1]
    eye = lax.broadcasted_iota(jnp.int32, (n, n), 0) == lax.broadcasted_iota(jnp.int32, (n, n), 1)
    return jnp.sum(jnp.where(eye, row, 0.0), axis=1, keepdims=True)


def pair_row(small_ref, at, seqs):
    return jnp.concatenate([small_ref[at : at + 1, 0:seqs], small_ref[at + 1 : at + 2, 0:seqs]], axis=1)


def slots_of(small_ref, experts, seqs):
    hit_row = pair_row(small_ref, ROUTES, seqs).astype(jnp.int32)
    pairs = hit_row.shape[1]
    hit = (lax.broadcasted_iota(jnp.int32, (experts, pairs), 0) == hit_row).astype(f32)
    upper = (
        lax.broadcasted_iota(jnp.int32, (pairs, pairs), 0)
        < lax.broadcasted_iota(jnp.int32, (pairs, pairs), 1)
    ).astype(bf16)
    before = nn(hit.astype(bf16), upper)
    slot = jnp.sum(before * hit, axis=0, keepdims=True).astype(jnp.int32)
    return hit_row * 2 + slot // 2, slot % 2


def route_tables(small_ref, disp_ref, comb_ref, w_ref):
    rows = disp_ref.shape[1]
    seqs = disp_ref.shape[2]
    place, half = slots_of(small_ref, rows // 2, seqs)
    at = lax.broadcasted_iota(jnp.int32, (rows, 2 * seqs), 0) == place
    place_col = as_column(place.astype(f32)).astype(jnp.int32)
    half_col = as_column(half.astype(f32)).astype(jnp.int32)
    at_col = lax.broadcasted_iota(jnp.int32, (2 * seqs, rows), 1) == place_col
    for j in (0, 1):
        table = (at & (half == j)).astype(f32)
        disp_ref[j] = (table[:, :seqs] + table[:, seqs:]).astype(bf16)
        comb_ref[j] = (at_col & (half_col == j)).astype(bf16)
    w_ref[...] = jnp.broadcast_to(as_column(pair_row(small_ref, WEIGHTS, seqs)), w_ref.shape)


def normed_rows(x_ref, small_ref, at, rows, tp):
    left = left_half((rows, 128))
    left_row = left_half((1, 128))
    total = jnp.zeros((rows, 128), f32)
    for i in range(tp):
        x = x_ref[rows * i : rows * (i + 1), :].astype(f32)
        total = total + x * x
    sums = [jnp.sum(jnp.where(left == keep, total, 0.0), axis=1, keepdims=True) for keep in (True, False)]
    scales = [lax.rsqrt(v / (64.0 * tp) + EPS) for v in sums]
    scale = jnp.where(left, scales[0], scales[1])
    tiles = []
    for i in range(tp // 2):
        gain = small_ref[at + i : at + i + 1, :]
        turned = swap(gain)
        gains = (jnp.where(left_row, gain, turned), jnp.where(left_row, turned, gain))
        a, b = [
            (x_ref[rows * (2 * i + j) : rows * (2 * i + j + 1), :].astype(f32) * scale * gains[j]).astype(bf16)
            for j in (0, 1)
        ]
        tiles.append(jnp.concatenate([jnp.where(left, a, swap(b)), jnp.where(left, swap(a), b)], axis=0))
    return jnp.concatenate(tiles, axis=1)


def qkv_kernel(x_ref, small_ref, wq_ref, wk_ref, wv_ref, o_ref, s_ref):
    rows = 16
    tp = x_ref.shape[0] // rows
    hidden = normed_rows(x_ref, small_ref, MIX, rows, tp)
    w = jnp.concatenate([wq_ref[...], wk_ref[...], wv_ref[...]], axis=0)
    out = nt(hidden, w)
    v = out[:, 128:192]
    s_ref[pl.ds(0, 32, stride=2), :] = out[:, :128]
    s_ref[pl.ds(1, 32, stride=2), :] = jnp.concatenate([v, jnp.zeros_like(v)], axis=1)
    o_ref[...] = s_ref[...].astype(bf16)


def attend_kernel(
    x_ref, small_ref, ck_ref, cv_ref, o_ref, nk_ref, nv_ref, disp_ref, comb_ref, w_ref,
    s_ref, p_ref,
):
    heads, length, width = ck_ref.shape
    s_ref[...] = x_ref[...].astype(f32)
    rows = 2 * heads
    qk_even = s_ref[pl.ds(0, rows, stride=4), :]
    v_even = s_ref[pl.ds(1, rows, stride=4), :]
    qk_odd = s_ref[pl.ds(2, rows, stride=4), :]
    v_odd = s_ref[pl.ds(3, rows, stride=4), :]
    left = left_half((rows, 128))
    q = jnp.where(left, qk_even, swap(qk_odd))
    k = jnp.where(left, swap(qk_even), qk_odd)
    v = jnp.where(left, v_even, swap(v_odd))

    def unit(z, gain):
        r = lax.rsqrt(jnp.mean(z * z, axis=1, keepdims=True) + EPS)
        return (z * r * gain).astype(bf16).astype(f32)

    qu = unit(q, small_ref[QG : QG + 1, :])
    ku = unit(k, small_ref[KG : KG + 1, :])
    s_ref[0:rows, :] = ku
    s_ref[rows : 2 * rows, :] = v
    new_key = jnp.concatenate(
        [s_ref[pl.ds(0, heads, stride=2), :], s_ref[pl.ds(1, heads, stride=2), :]], axis=1
    )
    new_value = jnp.concatenate(
        [s_ref[pl.ds(rows, heads, stride=2), :], s_ref[pl.ds(rows + 1, heads, stride=2), :]], axis=1
    )
    nk_ref[...] = new_key.astype(bf16)
    nv_ref[...] = new_value.astype(bf16)

    row = lax.broadcasted_iota(jnp.int32, (rows, 1), 0)
    first_map = (row % 2) == 0
    wide = jnp.concatenate(
        [jnp.where(first_map, qu, 0.0), jnp.where(first_map, 0.0, qu)], axis=1
    )
    wideb = wide.astype(bf16)
    scores = jnp.concatenate([nt(wideb[2 * h : 2 * h + 2], ck_ref[h]) for h in range(heads)], axis=0)
    scale = 128.0 ** -0.5
    scores = scores * scale
    own = jnp.sum(qu * ku, axis=1, keepdims=True) * scale
    live = lax.broadcasted_iota(jnp.int32, (rows, length), 1) < small_ref[LENGTH : LENGTH + 1, 0:1].astype(jnp.int32)
    scores = jnp.where(live, scores, MASKED)
    peak = jnp.maximum(jnp.max(scores, axis=1, keepdims=True), own)
    weight = jnp.exp(scores - peak)
    own_weight = jnp.exp(own - peak)
    totals = jnp.sum(weight, axis=1, keepdims=True) + own_weight
    prob = weight / totals
    p_ref[0] = prob[:, 0:128]
    p_ref[1] = jnp.concatenate([prob[:, 128:length], jnp.zeros((rows, 256 - length), f32)], axis=1)
    p_ref[2] = jnp.broadcast_to(own_weight / totals, (rows, 128))
    head = lax.broadcasted_iota(jnp.int32, (heads, 1), 0)
    lam = as_column(small_ref[LAM : LAM + 1, 0:heads])
    mixes = [
        p_ref[pl.ds(j, 1), pl.ds(0, heads, stride=2), :][0] - lam * p_ref[pl.ds(j, 1), pl.ds(1, heads, stride=2), :][0]
        for j in range(3)
    ]
    past_mix = jnp.concatenate(mixes[:2], axis=1)[:, 0:length]
    own_mix = mixes[2][:, 0:1].astype(bf16).astype(f32)
    mixb = past_mix.astype(bf16)
    out = own_mix * new_value.astype(bf16).astype(f32) + jnp.concatenate(
        [nn(mixb[h : h + 1], cv_ref[h]) for h in range(heads)], axis=0
    )
    r = lax.rsqrt(jnp.mean(out * out, axis=1, keepdims=True) + EPS)
    sub = jnp.concatenate([small_ref[SG : SG + 1, :], small_ref[SG + 1 : SG + 2, :]], axis=1)
    mixed = (out * r * sub * OUT_FACTOR).astype(bf16)
    route_tables(small_ref, disp_ref, comb_ref, w_ref)
    for i in range(o_ref.shape[0] // heads):
        o_ref[heads * i : heads * (i + 1), :] = mixed


def project_kernel(x_ref, w_ref, r_ref, disp_ref, u_ref, o_ref, s_ref):
    seqs = r_ref.shape[0]
    heads = x_ref.shape[0] // seqs
    width = x_ref.shape[1]
    for j in range(2):
        s_ref[j] = x_ref[:, 128 * j : 128 * (j + 1)].astype(f32)
    acc = r_ref[...].astype(f32)
    mixed = jnp.concatenate(
        [
            s_ref[pl.ds(j, 1), pl.ds(h, seqs, stride=heads), :][0].astype(bf16)
            for h in range(heads)
            for j in range(2)
        ],
        axis=1,
    )
    acc = acc + nt(mixed, w_ref[...])
    updated = acc.astype(bf16)
    u_ref[...] = updated
    halves = [nn(disp_ref[j], updated) for j in (0, 1)]
    o_ref[...] = jnp.concatenate(halves, axis=1).astype(bf16)


def expert_kernel(x_ref, small_ref, wg_ref, wu_ref, wd_ref, o_ref):
    rows = 64
    tp = x_ref.shape[0] // rows
    left = left_half((rows, 128))
    hidden = normed_rows(x_ref, small_ref, FFN, rows, tp)
    both = nn(hidden, jnp.concatenate([wg_ref[...], wu_ref[...]], axis=1))
    gate = both[:, :128]
    act = (gate / (1.0 + jnp.exp(-gate)) * both[:, 128:]).astype(bf16)
    for i in range(tp // 2):
        if i % 2 == 0:
            pair = nn(act, wd_ref[:, 128 * i : 128 * (i + 2)])
        out = pair[:, 128 * (i % 2) : 128 * (i % 2 + 1)].astype(bf16)
        a = out[:rows]
        b = out[rows:]
        o_ref[2 * rows * i : 2 * rows * i + rows, :] = jnp.where(left, a, swap(b))
        o_ref[2 * rows * i + rows : 2 * rows * (i + 1), :] = jnp.where(left, swap(a), b)


def sum_kernel(x_ref, o_ref):
    total = jnp.zeros(o_ref.shape, f32)
    rows = o_ref.shape[0]
    for i in range(x_ref.shape[0] // rows):
        total = total + x_ref[rows * i : rows * (i + 1), :].astype(f32)
    o_ref[...] = total.astype(bf16)


def combine_kernel(x_ref, u_ref, comb_ref, w_ref, key_ref, value_ref, o_ref, nk_ref, nv_ref):
    nk_ref[...] = key_ref[...]
    nv_ref[...] = value_ref[...]
    seqs = u_ref.shape[0]
    x = x_ref[...]
    picked = nn(comb_ref[0], x[:, :64]) + nn(comb_ref[1], x[:, 64:])
    picked = picked * w_ref[:, :64]
    out = u_ref[...].astype(f32) + (picked[:seqs] + picked[seqs:])
    o_ref[...] = out.astype(bf16)


def call(body, out, specs, scratch=(), name=None, flops=None):
    return pl.pallas_call(
        body,
        out_shape=out,
        in_specs=specs,
        out_specs=jax.tree.map(lambda _: VMEM, out),
        scratch_shapes=scratch,
        compiler_params=pltpu.CompilerParams(vmem_limit_bytes=8 * 1024 * 1024),
        name=name,
        cost_estimate=flops and pl.CostEstimate(flops=flops, bytes_accessed=0, transcendentals=0),
    )


def sds(shape, dtype=bf16):
    return jax.ShapeDtypeStruct(shape, dtype)


def broadcast(x, axis):
    n = lax.axis_size(axis)
    return jnp.broadcast_to(x, (n, *x.shape)).reshape(n * x.shape[0], x.shape[1])


def exchange(x, axis):
    n = lax.axis_size(axis)
    rows, lanes = x.shape
    out = lax.all_to_all(
        x.reshape(n, rows // n, lanes), axis, split_axis=0, concat_axis=0, tiled=True
    )
    return out.reshape(rows, lanes)


def local(
    resid, cache_key, cache_value, lengths, lambdas, mix_gain, query_gain, key_gain, sub_gain,
    ffn_gain, w_query, w_key, w_value, w_out, routes, route_weights, w_gate, w_up, w_down,
):
    length = call(lead_kernel, sds((8, 128), f32), [SMEM], name="lead", flops=3000000000)(lengths)
    packed, small = call(
        pack_kernel, (sds((512, 128)), sds((SMALL, 128), f32)), [VMEM] * 10, name="pack", flops=3000000000
    )(
        resid, mix_gain.reshape(16, 128), ffn_gain.reshape(16, 128), query_gain.reshape(1, 128),
        key_gain.reshape(1, 128), sub_gain.reshape(2, 128), lambdas.reshape(1, 8),
        length, routes.T, route_weights.T,
    )
    everyone = exchange(packed, "tp")
    qkv = call(
        qkv_kernel, sds((64, 128)), [VMEM] * 5, [pltpu.VMEM((64, 128), f32)], name="qkv", flops=3000000000
    )(everyone, small, w_query.T, w_key.T, w_value.T)
    mine = exchange(qkv, "tp")
    mixed, new_key, new_value, disp, comb, rw = call(
        attend_kernel,
        (
            sds((256, 256)), sds((8, 256)), sds((8, 256)),
            sds((2, 64, 32)), sds((2, 64, 64)), sds((64, 128), f32),
        ),
        [VMEM] * 4,
        [
            pltpu.VMEM((64, 128), f32),
            pltpu.VMEM((3, 16, 128), f32),
        ],
        name="attend",
        flops=3000000000,
    )(mine, small, cache_key[0], cache_value[0])
    heads = exchange(mixed, "tp")
    updated, send = call(
        project_kernel,
        (sds((32, 64)), sds((64, 128))),
        [VMEM] * 4,
        [pltpu.VMEM((2, 256, 128), f32)],
        name="project",
        flops=3000000000,
    )(heads, w_out.T, resid, disp)
    slots = exchange(send, "ep")
    slot_rows = exchange(broadcast(slots, "tp"), "tp")
    partial = call(expert_kernel, sds((2048, 128)), [VMEM] * 5, name="expert", flops=3000000000)(
        slot_rows, small, w_gate[0], w_up[0], w_down[0]
    )
    arrived = exchange(partial, "tp")
    summed = call(sum_kernel, sds((64, 128)), [VMEM], name="sum", flops=3000000000)(arrived)
    returned = exchange(summed, "ep")
    result, new_key, new_value = call(
        combine_kernel, (sds((32, 64)), sds((8, 256)), sds((8, 256))), [VMEM] * 6, name="combine"
    )(returned, updated, comb, rw, new_key, new_value)
    return (result, new_key[None], new_value[None])


def solution(mesh):
    in_specs = (
        P("ep", "tp"),
        P(("ep", "tp"), None, None, None),
        P(("ep", "tp"), None, None, None),
        P(("ep", "tp")),
        P(), P(), P(), P(), P(), P(),
        P(None, "tp"),
        P(None, "tp"),
        P(None, "tp"),
        P(None, "tp"),
        P("ep", None),
        P("ep", None),
        P("ep", None, "tp"),
        P("ep", None, "tp"),
        P("ep", "tp", None),
    )
    out_specs = (P("ep", "tp"), P(("ep", "tp"), None, None), P(("ep", "tp"), None, None))
    return jax.shard_map(local, mesh=mesh, in_specs=in_specs, out_specs=out_specs, check_vma=False)
```

```python
import math

import jax
import jax.numpy as jnp
from jax import lax
from jax.experimental import pallas as pl
from jax.experimental.pallas import tpu as pltpu
from jax.sharding import PartitionSpec as P

CAP = 4
EPS = 1e-06
OUT_FACTOR = 0.2 + 0.6 * math.exp(-0.3)
MASKED = -1e30

f32 = jnp.float32
bf16 = jnp.bfloat16

VMEM = pl.BlockSpec(memory_space=pltpu.VMEM)
SMEM = pl.BlockSpec(memory_space=pltpu.SMEM)
HBM = pl.BlockSpec(memory_space=pltpu.HBM)


def nt(a, b):
    return lax.dot_general(a, b, (((1,), (1,)), ((), ())), preferred_element_type=f32)


def nn(a, b):
    return lax.dot_general(a, b, (((1,), (0,)), ((), ())), preferred_element_type=f32)


def tn(a, b):
    return lax.dot_general(a, b, (((0,), (0,)), ((), ())), preferred_element_type=f32)


def left_half(shape):
    return lax.broadcasted_iota(jnp.int32, shape, len(shape) - 1) < 64


def swap(x):
    return pltpu.roll(x, 64, 1)


MIX, FFN, QG, KG, SG, LAM, LENGTH, ROUTES, WEIGHTS, SMALL = 0, 16, 32, 33, 34, 36, 37, 38, 40, 48


def lead_kernel(len_ref, o_ref):
    o_ref[...] = jnp.full(o_ref.shape, len_ref[0], jnp.int32).astype(f32)


def pack_kernel(x_ref, mix_ref, ffn_ref, qg_ref, kg_ref, sg_ref, lam_ref, len_ref, routes_ref, rw_ref, o_ref, small_ref):
    small_ref[...] = jnp.zeros(small_ref.shape, f32)
    small_ref[MIX:FFN, :] = mix_ref[...]
    small_ref[FFN:QG, :] = ffn_ref[...]
    small_ref[QG : QG + 1, :] = qg_ref[...]
    small_ref[KG : KG + 1, :] = kg_ref[...]
    small_ref[SG : SG + 2, :] = sg_ref[...]
    small_ref[LAM : LAM + 1, 0 : lam_ref.shape[1]] = lam_ref[...]
    small_ref[LENGTH : LENGTH + 1, :] = len_ref[0:1, :]
    small_ref[ROUTES : ROUTES + 2, 0 : routes_ref.shape[1]] = routes_ref[...].astype(f32)
    small_ref[WEIGHTS : WEIGHTS + 2, 0 : rw_ref.shape[1]] = rw_ref[...]
    x = x_ref[...].astype(f32)
    packed = jnp.concatenate([x[:16], x[16:]], axis=1).astype(bf16)
    for i in range(o_ref.shape[0] // 16):
        o_ref[16 * i : 16 * (i + 1), :] = packed


def as_column(row):
    n = row.shape[1]
    eye = lax.broadcasted_iota(jnp.int32, (n, n), 0) == lax.broadcasted_iota(jnp.int32, (n, n), 1)
    return jnp.sum(jnp.where(eye, row, 0.0), axis=1, keepdims=True)


def pair_row(small_ref, at, seqs):
    return jnp.concatenate([small_ref[at : at + 1, 0:seqs], small_ref[at + 1 : at + 2, 0:seqs]], axis=1)


def slots_of(small_ref, experts, seqs):
    hit_row = pair_row(small_ref, ROUTES, seqs).astype(jnp.int32)
    pairs = hit_row.shape[1]
    hit = (lax.broadcasted_iota(jnp.int32, (experts, pairs), 0) == hit_row).astype(f32)
    upper = (
        lax.broadcasted_iota(jnp.int32, (pairs, pairs), 0)
        < lax.broadcasted_iota(jnp.int32, (pairs, pairs), 1)
    ).astype(bf16)
    before = nn(hit.astype(bf16), upper)
    slot = jnp.sum(before * hit, axis=0, keepdims=True).astype(jnp.int32)
    return hit_row * 2 + slot // 2, slot % 2


def route_tables(small_ref, disp_ref, comb_ref, w_ref):
    rows = disp_ref.shape[1]
    seqs = disp_ref.shape[2]
    place, half = slots_of(small_ref, rows // 2, seqs)
    at = lax.broadcasted_iota(jnp.int32, (rows, 2 * seqs), 0) == place
    place_col = as_column(place.astype(f32)).astype(jnp.int32)
    half_col = as_column(half.astype(f32)).astype(jnp.int32)
    at_col = lax.broadcasted_iota(jnp.int32, (2 * seqs, rows), 1) == place_col
    for j in (0, 1):
        table = (at & (half == j)).astype(f32)
        disp_ref[j] = (table[:, :seqs] + table[:, seqs:]).astype(bf16)
        comb_ref[j] = (at_col & (half_col == j)).astype(bf16)
    w_ref[...] = jnp.broadcast_to(as_column(pair_row(small_ref, WEIGHTS, seqs)), w_ref.shape)


def normed_rows(x_ref, small_ref, at, rows, tp):
    left = left_half((rows, 128))
    left_row = left_half((1, 128))
    total = jnp.zeros((rows, 128), f32)
    for i in range(tp):
        x = x_ref[rows * i : rows * (i + 1), :].astype(f32)
        total = total + x * x
    sums = [jnp.sum(jnp.where(left == keep, total, 0.0), axis=1, keepdims=True) for keep in (True, False)]
    scales = [lax.rsqrt(v / (64.0 * tp) + EPS) for v in sums]
    scale = jnp.where(left, scales[0], scales[1])
    tiles = []
    for i in range(tp // 2):
        gain = small_ref[at + i : at + i + 1, :]
        turned = swap(gain)
        gains = (jnp.where(left_row, gain, turned), jnp.where(left_row, turned, gain))
        a, b = [
            (x_ref[rows * (2 * i + j) : rows * (2 * i + j + 1), :].astype(f32) * scale * gains[j]).astype(bf16)
            for j in (0, 1)
        ]
        tiles.append(jnp.concatenate([jnp.where(left, a, swap(b)), jnp.where(left, swap(a), b)], axis=0))
    return jnp.concatenate(tiles, axis=1)


def qkv_kernel(x_ref, small_ref, wq_ref, wk_ref, wv_ref, o_ref, s_ref):
    rows = 16
    tp = x_ref.shape[0] // rows
    hidden = normed_rows(x_ref, small_ref, MIX, rows, tp)
    w = jnp.concatenate([wq_ref[...], wk_ref[...], wv_ref[...]], axis=0)
    out = nt(hidden, w)
    v = out[:, 128:192]
    s_ref[pl.ds(0, 32, stride=2), :] = out[:, :128]
    s_ref[pl.ds(1, 32, stride=2), :] = jnp.concatenate([v, jnp.zeros_like(v)], axis=1)
    o_ref[...] = s_ref[...].astype(bf16)


def attend_kernel(
    x_ref, small_ref, ck_ref, cv_ref, o_ref, nk_ref, nv_ref, disp_ref, comb_ref, w_ref,
    s_ref, p_ref,
):
    heads, length, width = ck_ref.shape
    s_ref[...] = x_ref[...].astype(f32)
    rows = 2 * heads
    qk_even = s_ref[pl.ds(0, rows, stride=4), :]
    v_even = s_ref[pl.ds(1, rows, stride=4), :]
    qk_odd = s_ref[pl.ds(2, rows, stride=4), :]
    v_odd = s_ref[pl.ds(3, rows, stride=4), :]
    left = left_half((rows, 128))
    q = jnp.where(left, qk_even, swap(qk_odd))
    k = jnp.where(left, swap(qk_even), qk_odd)
    v = jnp.where(left, v_even, swap(v_odd))

    def unit(z, gain):
        r = lax.rsqrt(jnp.mean(z * z, axis=1, keepdims=True) + EPS)
        return (z * r * gain).astype(bf16).astype(f32)

    qu = unit(q, small_ref[QG : QG + 1, :])
    ku = unit(k, small_ref[KG : KG + 1, :])
    s_ref[0:rows, :] = ku
    s_ref[rows : 2 * rows, :] = v
    new_key = jnp.concatenate(
        [s_ref[pl.ds(0, heads, stride=2), :], s_ref[pl.ds(1, heads, stride=2), :]], axis=1
    )
    new_value = jnp.concatenate(
        [s_ref[pl.ds(rows, heads, stride=2), :], s_ref[pl.ds(rows + 1, heads, stride=2), :]], axis=1
    )
    nk_ref[...] = new_key.astype(bf16)
    nv_ref[...] = new_value.astype(bf16)

    row = lax.broadcasted_iota(jnp.int32, (rows, 1), 0)
    first_map = (row % 2) == 0
    wide = jnp.concatenate(
        [jnp.where(first_map, qu, 0.0), jnp.where(first_map, 0.0, qu)], axis=1
    )
    wideb = wide.astype(bf16)
    scores = jnp.concatenate([nt(wideb[2 * h : 2 * h + 2], ck_ref[h]) for h in range(heads)], axis=0)
    scale = 128.0 ** -0.5
    scores = scores * scale
    own = jnp.sum(qu * ku, axis=1, keepdims=True) * scale
    live = lax.broadcasted_iota(jnp.int32, (rows, length), 1) < small_ref[LENGTH : LENGTH + 1, 0:1].astype(jnp.int32)
    scores = jnp.where(live, scores, MASKED)
    peak = jnp.maximum(jnp.max(scores, axis=1, keepdims=True), own)
    weight = jnp.exp(scores - peak)
    own_weight = jnp.exp(own - peak)
    totals = jnp.sum(weight, axis=1, keepdims=True) + own_weight
    prob = weight / totals
    p_ref[0] = prob[:, 0:128]
    p_ref[1] = jnp.concatenate([prob[:, 128:length], jnp.zeros((rows, 256 - length), f32)], axis=1)
    p_ref[2] = jnp.broadcast_to(own_weight / totals, (rows, 128))
    head = lax.broadcasted_iota(jnp.int32, (heads, 1), 0)
    lam = as_column(small_ref[LAM : LAM + 1, 0:heads])
    mixes = [
        p_ref[pl.ds(j, 1), pl.ds(0, heads, stride=2), :][0] - lam * p_ref[pl.ds(j, 1), pl.ds(1, heads, stride=2), :][0]
        for j in range(3)
    ]
    past_mix = jnp.concatenate(mixes[:2], axis=1)[:, 0:length]
    own_mix = mixes[2][:, 0:1].astype(bf16).astype(f32)
    mixb = past_mix.astype(bf16)
    out = own_mix * new_value.astype(bf16).astype(f32) + jnp.concatenate(
        [nn(mixb[h : h + 1], cv_ref[h]) for h in range(heads)], axis=0
    )
    r = lax.rsqrt(jnp.mean(out * out, axis=1, keepdims=True) + EPS)
    sub = jnp.concatenate([small_ref[SG : SG + 1, :], small_ref[SG + 1 : SG + 2, :]], axis=1)
    mixed = (out * r * sub * OUT_FACTOR).astype(bf16)
    route_tables(small_ref, disp_ref, comb_ref, w_ref)
    for i in range(o_ref.shape[0] // heads):
        o_ref[heads * i : heads * (i + 1), :] = mixed


def project_kernel(x_ref, w_ref, r_ref, disp_ref, u_ref, o_ref, s_ref):
    seqs = r_ref.shape[0]
    heads = x_ref.shape[0] // seqs
    width = x_ref.shape[1]
    for j in range(2):
        s_ref[j] = x_ref[:, 128 * j : 128 * (j + 1)].astype(f32)
    acc = r_ref[...].astype(f32)
    mixed = jnp.concatenate(
        [
            s_ref[pl.ds(j, 1), pl.ds(h, seqs, stride=heads), :][0].astype(bf16)
            for h in range(heads)
            for j in range(2)
        ],
        axis=1,
    )
    acc = acc + nt(mixed, w_ref[...])
    updated = acc.astype(bf16)
    u_ref[...] = updated
    halves = [nn(disp_ref[j], updated) for j in (0, 1)]
    o_ref[...] = jnp.concatenate(halves, axis=1).astype(bf16)


def expert_kernel(x_ref, small_ref, wg_ref, wu_ref, wd_ref, o_ref):
    rows = 64
    tp = x_ref.shape[0] // rows
    left = left_half((rows, 128))
    hidden = normed_rows(x_ref, small_ref, FFN, rows, tp)
    gate = nn(hidden, wg_ref[...])
    up = nn(hidden, wu_ref[...])
    act = (gate / (1.0 + jnp.exp(-gate)) * up).astype(bf16)
    for i in range(tp // 2):
        if i % 2 == 0:
            pair = nn(act, wd_ref[:, 128 * i : 128 * (i + 2)])
        out = pair[:, 128 * (i % 2) : 128 * (i % 2 + 1)].astype(bf16)
        a = out[:rows]
        b = out[rows:]
        o_ref[2 * rows * i : 2 * rows * i + rows, :] = jnp.where(left, a, swap(b))
        o_ref[2 * rows * i + rows : 2 * rows * (i + 1), :] = jnp.where(left, swap(a), b)


def sum_kernel(x_ref, o_ref):
    total = jnp.zeros(o_ref.shape, f32)
    rows = o_ref.shape[0]
    for i in range(x_ref.shape[0] // rows):
        total = total + x_ref[rows * i : rows * (i + 1), :].astype(f32)
    o_ref[...] = total.astype(bf16)


def combine_kernel(x_ref, u_ref, comb_ref, w_ref, key_ref, value_ref, o_ref, nk_ref, nv_ref):
    nk_ref[...] = key_ref[...]
    nv_ref[...] = value_ref[...]
    seqs = u_ref.shape[0]
    x = x_ref[...]
    picked = nn(comb_ref[0], x[:, :64]) + nn(comb_ref[1], x[:, 64:])
    picked = picked * w_ref[:, :64]
    out = u_ref[...].astype(f32) + (picked[:seqs] + picked[seqs:])
    o_ref[...] = out.astype(bf16)


def call(body, out, specs, scratch=(), name=None, flops=None):
    return pl.pallas_call(
        body,
        out_shape=out,
        in_specs=specs,
        out_specs=jax.tree.map(lambda _: VMEM, out),
        scratch_shapes=scratch,
        compiler_params=pltpu.CompilerParams(vmem_limit_bytes=8 * 1024 * 1024),
        name=name,
        cost_estimate=flops and pl.CostEstimate(flops=flops, bytes_accessed=0, transcendentals=0),
    )


def sds(shape, dtype=bf16):
    return jax.ShapeDtypeStruct(shape, dtype)


def broadcast(x, axis):
    n = lax.axis_size(axis)
    return jnp.broadcast_to(x, (n, *x.shape)).reshape(n * x.shape[0], x.shape[1])


def exchange(x, axis):
    n = lax.axis_size(axis)
    rows, lanes = x.shape
    out = lax.all_to_all(
        x.reshape(n, rows // n, lanes), axis, split_axis=0, concat_axis=0, tiled=True
    )
    return out.reshape(rows, lanes)


def local(
    resid, cache_key, cache_value, lengths, lambdas, mix_gain, query_gain, key_gain, sub_gain,
    ffn_gain, w_query, w_key, w_value, w_out, routes, route_weights, w_gate, w_up, w_down,
):
    length = call(lead_kernel, sds((8, 128), f32), [SMEM], name="lead", flops=3000000000)(lengths)
    packed, small = call(
        pack_kernel, (sds((512, 128)), sds((SMALL, 128), f32)), [VMEM] * 10, name="pack", flops=3000000000
    )(
        resid, mix_gain.reshape(16, 128), ffn_gain.reshape(16, 128), query_gain.reshape(1, 128),
        key_gain.reshape(1, 128), sub_gain.reshape(2, 128), lambdas.reshape(1, 8),
        length, routes.T, route_weights.T,
    )
    everyone = exchange(packed, "tp")
    qkv = call(
        qkv_kernel, sds((64, 128)), [VMEM] * 5, [pltpu.VMEM((64, 128), f32)], name="qkv", flops=3000000000
    )(everyone, small, w_query.T, w_key.T, w_value.T)
    mine = exchange(qkv, "tp")
    mixed, new_key, new_value, disp, comb, rw = call(
        attend_kernel,
        (
            sds((256, 256)), sds((8, 256)), sds((8, 256)),
            sds((2, 64, 32)), sds((2, 64, 64)), sds((64, 128), f32),
        ),
        [VMEM] * 4,
        [
            pltpu.VMEM((64, 128), f32),
            pltpu.VMEM((3, 16, 128), f32),
        ],
        name="attend",
        flops=3000000000,
    )(mine, small, cache_key[0], cache_value[0])
    heads = exchange(mixed, "tp")
    updated, send = call(
        project_kernel,
        (sds((32, 64)), sds((64, 128))),
        [VMEM] * 4,
        [pltpu.VMEM((2, 256, 128), f32)],
        name="project",
        flops=3000000000,
    )(heads, w_out.T, resid, disp)
    slots = exchange(send, "ep")
    slot_rows = exchange(broadcast(slots, "tp"), "tp")
    partial = call(expert_kernel, sds((2048, 128)), [VMEM] * 5, name="expert", flops=3000000000)(
        slot_rows, small, w_gate[0], w_up[0], w_down[0]
    )
    arrived = exchange(partial, "tp")
    summed = call(sum_kernel, sds((64, 128)), [VMEM], name="sum", flops=3000000000)(arrived)
    returned = exchange(summed, "ep")
    result, new_key, new_value = call(
        combine_kernel, (sds((32, 64)), sds((8, 256)), sds((8, 256))), [VMEM] * 6, name="combine"
    )(returned, updated, comb, rw, new_key, new_value)
    return (result, new_key[None], new_value[None])


def solution(mesh):
    in_specs = (
        P("ep", "tp"),
        P(("ep", "tp"), None, None, None),
        P(("ep", "tp"), None, None, None),
        P(("ep", "tp")),
        P(), P(), P(), P(), P(), P(),
        P(None, "tp"),
        P(None, "tp"),
        P(None, "tp"),
        P(None, "tp"),
        P("ep", None),
        P("ep", None),
        P("ep", None, "tp"),
        P("ep", None, "tp"),
        P("ep", "tp", None),
    )
    out_specs = (P("ep", "tp"), P(("ep", "tp"), None, None), P(("ep", "tp"), None, None))
    return jax.shard_map(local, mesh=mesh, in_specs=in_specs, out_specs=out_specs, check_vma=False)
```
